32 devices in a mesh: sp: 8 (over z, x), tp: 4 (over y, core).
Axes of the slice: x: 2, y: 2, z: 4, core: 2. Of those that a mesh axis runs over, the one named last changes fastest.
Arguments:
- token_grid: bfloat16 [8, 2048, 512], P('sp', 'tp'), may hold values from -6 to 6
- norm_gain: bfloat16 [3, 2048], replicated, may hold values from 0.099609375 to 1.8984375
- w_query: bfloat16 [3, 2048, 2048], P(None, None, 'tp'), may hold values from -0.125 to 0.125
- w_key: bfloat16 [3, 2048, 2048], P(None, None, 'tp'), may hold values from -0.125 to 0.125
- w_value: bfloat16 [3, 2048, 2048], P(None, None, 'tp'), may hold values from -0.125 to 0.125
- w_out: bfloat16 [3, 2048, 2048], P(None, 'tp'), may hold values from -0.5 to 0.5
- rel_bias: float32 [3, 32, 8, 16], P(None, 'tp'), may hold values from -3 to 250
Outputs:
- grid_out: bfloat16 [8, 2048, 512], P('sp', 'tp')
The draws below stay inside these ranges and needn't reach their ends.
All inputs are finite; a program needn't handle non-finite values.
Results may differ from the reference program's by a relative error of at most 0.024.
Values may be sent and summed in bfloat16 or wider, within the bound.
A program may use at most 128 MiB of HBM per device.

```python
import jax
import jax.numpy as jnp
from jax import lax

D = 2048
HEADS = 32
HEAD_DIM = 64
WIN_R = 8
WIN_C = 16
LAYERS = 3
COLS = 512
ROWS = 8
N_TP = 4


def draw_rel_bias(key, part):
    dims_all = (LAYERS, HEADS, WIN_R, WIN_C)
    baseline = jnp.clip(jax.random.normal(jax.random.fold_in(key, 11), dims_all, jnp.float32), -3.0, 3.0)
    return baseline


def block_scale(own_key, shape, shards, low, high):
    def one(axis_at, shards_of):
        steps = jax.random.uniform(jax.random.fold_in(jax.random.fold_in(own_key, 6), axis_at), (shards_of,), jnp.float32, low / len(shards), high / len(shards))
        return jnp.repeat(jnp.exp(steps), shape[axis_at] // shards_of).reshape((-1,) + (1,) * (len(shape) - axis_at - 1))

    factor_of = one(*shards[0])
    for cut in shards[1:]:
        factor_of = factor_of * one(*cut)
    return factor_of


def scatter_about(key, dims, deviation, most, pieces=(), kind=jnp.bfloat16):
    drawn = deviation * jax.random.normal(key, dims, jnp.float32)
    if pieces:
        drawn = drawn * block_scale(key, dims, pieces, -0.22, 0.18)
    return jnp.clip(drawn, -most, most).astype(kind)


def setup_inputs(seed: int = 0) -> dict:
    keys = jax.random.split(jax.random.key(seed), 8)
    return {
        "token_grid": scatter_about(keys[0], (ROWS, D, COLS), 1.0, 6.0, ((0, 8), (1, 4))),
        "norm_gain": jnp.clip(1.0 + 0.18 * jax.random.normal(keys[1], (LAYERS, D), jnp.float32), 0.099609375, 1.8984375).astype(jnp.bfloat16),
        "w_query": scatter_about(keys[2], (LAYERS, D, D), D ** -0.5, 0.125, ((2, 4),)),
        "w_key": scatter_about(keys[3], (LAYERS, D, D), D ** -0.5, 0.125, ((2, 4),)),
        "w_value": scatter_about(keys[4], (LAYERS, D, D), D ** -0.5, 0.125, ((2, 4),)),
        "w_out": scatter_about(keys[5], (LAYERS, D, D), (D // 16) ** -0.5, 0.5, ((1, 4),)),
        "rel_bias": draw_rel_bias(jax.random.fold_in(keys[7], 71), 0),
    }


EPS = 1e-06

def rounded(source):
    return lax.optimization_barrier(source.astype(jnp.bfloat16)).astype(jnp.float32)

def one_layer(token_grid, gain_row, w_query, w_key, w_value, w_out, bias_table):
    grid_wide = token_grid.astype(jnp.float32)
    inverse = lax.rsqrt(lax.optimization_barrier(jnp.mean(grid_wide * grid_wide, axis=1)) + EPS)
    scaled = (grid_wide * gain_row.astype(jnp.float32)[None, :, None]).astype(jnp.bfloat16)
    flat_rows = jnp.transpose(scaled, (0, 2, 1)).reshape(ROWS * COLS, D)
    inverse_flat = inverse.reshape(ROWS * COLS, 1)

    def project(weight):
        product = jnp.dot(flat_rows, weight, preferred_element_type=jnp.float32) * inverse_flat
        return rounded(product).reshape(ROWS, COLS, HEADS, HEAD_DIM)
    queries = project(w_query)
    keys_all = project(w_key)
    values_all = project(w_value)
    factor = HEAD_DIM ** (-0.5)
    offsets = jnp.arange(WIN_R * WIN_C, dtype=jnp.int32)

    def scores_at(offset):
        slot_row = offset // WIN_C
        slot_col = offset % WIN_C
        rolled = jnp.roll(keys_all, (WIN_R // 2 - slot_row, WIN_C // 2 - slot_col), axis=(0, 1))
        offset_bias = lax.dynamic_slice(bias_table, (jnp.int32(0), slot_row, slot_col), (HEADS, 1, 1)).reshape(HEADS)
        return lax.optimization_barrier(jnp.sum(queries * rolled, axis=-1)) * factor + offset_bias
    scores = lax.map(scores_at, offsets)
    weights = rounded(jax.nn.softmax(scores, axis=0))

    def accumulate(running, operands):
        weight_now, offset = operands
        slot_row = offset // WIN_C
        slot_col = offset % WIN_C
        rolled = jnp.roll(values_all, (WIN_R // 2 - slot_row, WIN_C // 2 - slot_col), axis=(0, 1))
        return (running + weight_now[..., None] * rolled, None)
    mixed_out, unused = lax.scan(accumulate, jnp.zeros((ROWS, COLS, HEADS, HEAD_DIM), jnp.float32), (weights, offsets))
    mixed_out = mixed_out.astype(jnp.bfloat16).reshape(ROWS * COLS, N_TP, D // N_TP)
    groups = jnp.moveaxis(mixed_out, 1, 0)
    blocks = w_out.reshape(N_TP, D // N_TP, D)

    def add_group(running, operands):
        partial_value = jnp.dot(operands[0], operands[1], preferred_element_type=jnp.float32)
        return (running + rounded(partial_value), None)
    update, unused = lax.scan(add_group, jnp.zeros((ROWS * COLS, D), jnp.float32), (groups, blocks))
    update = jnp.transpose(update.reshape(ROWS, COLS, D), (0, 2, 1))
    return (grid_wide + update).astype(jnp.bfloat16)

def reference(token_grid, norm_gain, w_query, w_key, w_value, w_out, rel_bias):
    current = token_grid
    for layer_idx in range(LAYERS):
        current = one_layer(current, norm_gain[layer_idx], w_query[layer_idx], w_key[layer_idx], w_value[layer_idx], w_out[layer_idx], rel_bias[layer_idx])
    return current
```

```python
import functools

import jax
import jax.numpy as jnp
from jax import lax
from jax.experimental import pallas as pl
from jax.experimental.pallas import tpu as pltpu
from jax.sharding import PartitionSpec as P

HEAD_DIM = 64
WIN_R = 8
WIN_C = 16
EPS = 1e-06
LANES = 128
NEG = -1e30
MESH = pl.DeviceIdType.MESH


def attention_kernel(rows, cols, q_ref, k_ref, v_ref, kh_ref, vh_ref, base_ref, o_ref, tile_ref):
    pack = LANES // cols
    n_slots = min(rows, pack + WIN_R - 1)
    half_r = WIN_R // 2
    span = cols + WIN_C
    lane = lax.broadcasted_iota(jnp.int32, (8, LANES), 1)
    lane_q = lax.broadcasted_iota(jnp.int32, (LANES, LANES), 1)
    v_main = v_ref[...].T
    v_halo = vh_ref[...].T
    neg = jnp.full((8, LANES), NEG, jnp.float32)
    outs = [[] for _ in range(rows * cols // LANES)]
    for head in range(LANES // HEAD_DIM):
        for p in range(pack):
            own = (lane >= p * cols) & (lane < (p + 1) * cols)
            for slot in range(WIN_R):
                e = (slot + p) % rows
                start = jnp.broadcast_to(base_ref[head, slot : slot + 1, :], (8, LANES))
                start = pltpu.roll(start, 0, 1, stride=1, stride_axis=0)
                for blk in range(span // 8):
                    shift = (p * cols + 8 * blk) % LANES
                    moved = pltpu.roll(start, shift, 1) if shift else start
                    at = blk - 1 if 1 <= blk <= cols // 8 else (cols // 8 if blk == 0 else blk)
                    where = pl.ds(e * span + 8 * at, 8)
                    rest = neg if p == 0 and rows == WIN_R else tile_ref[where, :]
                    tile_ref[where, :] = jnp.where(own, moved, rest)
        for group in range(rows * cols // LANES):
            key_rows = [r for r in range(rows) if (r - group * pack + half_r) % rows < n_slots]
            q = q_ref[group * LANES : (group + 1) * LANES, :]
            mine = (lane_q >= head * HEAD_DIM) & (lane_q < (head + 1) * HEAD_DIM)
            q = jnp.where(mine, q, jnp.zeros_like(q))
            s_list = []
            contract = (((1,), (1,)), ((), ()))
            if len(key_rows) == rows:
                s_main = lax.dot_general(k_ref[...], q, contract, preferred_element_type=jnp.float32)
                s_halo = lax.dot_general(kh_ref[...], q, contract, preferred_element_type=jnp.float32)
            main_list = []
            halo_list = []
            for r in key_rows:
                e = (r - group * pack + half_r) % rows
                if len(key_rows) == rows:
                    main = s_main[r * cols : (r + 1) * cols]
                    halo = s_halo[r * WIN_C : (r + 1) * WIN_C]
                else:
                    main = lax.dot_general(
                        k_ref[r * cols : (r + 1) * cols, :], q, contract, preferred_element_type=jnp.float32
                    )
                    halo = lax.dot_general(
                        kh_ref[r * WIN_C : (r + 1) * WIN_C, :], q, contract, preferred_element_type=jnp.float32
                    )
                main_list.append(main + tile_ref[e * span : e * span + cols, :])
                halo_list.append(halo + tile_ref[e * span + cols : (e + 1) * span, :])
            main = jnp.concatenate(main_list, axis=0)
            halo = jnp.concatenate(halo_list, axis=0)
            top = jnp.maximum(jnp.max(main, axis=0, keepdims=True), jnp.max(halo, axis=0, keepdims=True))
            main = jnp.exp(main - top)
            halo = jnp.exp(halo - top)
            total = jnp.sum(main, axis=0, keepdims=True) + jnp.sum(halo, axis=0, keepdims=True)
            main = main.astype(jnp.bfloat16)
            halo = halo.astype(jnp.bfloat16)
            lo = head * HEAD_DIM
            if len(key_rows) == rows:
                vm = v_main[lo : lo + HEAD_DIM]
                vh = v_halo[lo : lo + HEAD_DIM]
            else:
                vm = jnp.concatenate([v_main[lo : lo + HEAD_DIM, r * cols : (r + 1) * cols] for r in key_rows], axis=1)
                vh = jnp.concatenate(
                    [v_halo[lo : lo + HEAD_DIM, r * WIN_C : (r + 1) * WIN_C] for r in key_rows], axis=1
                )
            mixed = jnp.dot(vm, main, preferred_element_type=jnp.float32)
            mixed = mixed + jnp.dot(vh, halo, preferred_element_type=jnp.float32)
            outs[group].append(mixed / total)
    for group in range(rows * cols // LANES):
        both = jnp.concatenate(outs[group], axis=0)
        o_ref[group * LANES : (group + 1) * LANES, :] = both.T.astype(o_ref.dtype)


def attention_kernel_init(rows, cols, *refs):
    tile_ref = refs[-1]
    tile_ref[...] = jnp.full(tile_ref.shape, NEG, jnp.float32)
    attention_kernel(rows, cols, *refs)


def attention(queries, keys, values, halo, base, rows, cols):
    tokens, channels = queries.shape
    n_slots = min(rows, LANES // cols + WIN_R - 1)
    pairs = channels // LANES
    per = LANES // HEAD_DIM
    side = halo.shape[0]
    kernel = attention_kernel if rows == WIN_R else attention_kernel_init
    return pl.pallas_call(
        functools.partial(kernel, rows, cols),
        grid=(pairs,),
        out_shape=jax.ShapeDtypeStruct((tokens, channels), jnp.bfloat16),
        in_specs=[
            pl.BlockSpec((tokens, LANES), lambda i: (0, i)),
            pl.BlockSpec((tokens, LANES), lambda i: (0, i)),
            pl.BlockSpec((tokens, LANES), lambda i: (0, i)),
            pl.BlockSpec((side, LANES), lambda i: (0, i)),
            pl.BlockSpec((side, LANES), lambda i: (0, i + pairs)),
            pl.BlockSpec((per, WIN_R, LANES), lambda i: (i, 0, 0)),
        ],
        out_specs=pl.BlockSpec((tokens, LANES), lambda i: (0, i)),
        scratch_shapes=[pltpu.VMEM((n_slots * (cols + WIN_C), LANES), jnp.float32)],
        compiler_params=pltpu.CompilerParams(vmem_limit_bytes=48 * 1024 * 1024),
        name="window_attention",
    )(queries, keys, values, halo, halo, base)


def body(token_grid, norm_gain, w_query, w_key, w_value, w_out, rel_bias):
    n = lax.axis_size("sp")
    rows_dev, channels, columns = token_grid.shape
    rows = rows_dev * n
    cols = columns // n
    tokens = rows * cols
    width = norm_gain.shape[1]
    factor = HEAD_DIM ** (-0.5)
    half_c = WIN_C // 2
    base = jnp.concatenate(
        [
            rel_bias[..., :1],
            jnp.full(rel_bias.shape[:-1] + (LANES - WIN_C,), NEG, jnp.float32),
            jnp.flip(rel_bias[..., 1:], axis=-1),
        ],
        axis=-1,
    )
    turned = jnp.transpose(token_grid, (2, 0, 1)).reshape(columns, rows_dev * channels)
    current = lax.all_to_all(turned, "sp", split_axis=0, concat_axis=0, tiled=True)
    to_right = [(i, (i + 1) % n) for i in range(n)]
    to_left = [(i, (i - 1) % n) for i in range(n)]
    for layer in range(norm_gain.shape[0]):
        gain = norm_gain[layer].astype(jnp.float32)
        raw = lax.all_gather(current, "tp", axis=1, tiled=True).astype(jnp.float32)
        scaled = (raw * gain[None, :]).astype(jnp.bfloat16)
        inverse = lax.rsqrt(jnp.sum(raw * raw, axis=1, keepdims=True) / width + EPS)

        def project(weight, scale=1.0):
            product = jnp.dot(scaled, weight[layer], preferred_element_type=jnp.float32)
            return (product * inverse).astype(jnp.bfloat16) * jnp.bfloat16(scale)

        keys = project(w_key)
        values = project(w_value)
        keyval = jnp.concatenate([keys, values], axis=1).reshape(rows, cols, 2 * channels)
        left = lax.ppermute(keyval[:, cols - half_c :], "sp", to_right)
        right = lax.ppermute(keyval[:, :half_c], "sp", to_left)
        queries = project(w_query, factor)
        halo = jnp.concatenate([left, right], axis=1).reshape(rows * WIN_C, 2 * channels)
        mixed = attention(queries, keys, values, halo, base[layer], rows, cols)
        partial = jnp.dot(mixed, w_out[layer], preferred_element_type=jnp.float32).astype(jnp.bfloat16)
        update = lax.psum_scatter(partial, "tp", scatter_dimension=1, tiled=True)
        current = (current.astype(jnp.float32) + update.astype(jnp.float32)).astype(jnp.bfloat16)
    back = lax.all_to_all(current, "sp", split_axis=0, concat_axis=0, tiled=True)
    return jnp.transpose(back.reshape(columns, rows_dev, channels), (1, 2, 0))

def mega_kernel(cfg, *refs):
    layers, n, chunks, ccols, chan, heads, width = cfg
    (xt, gain, base, wq, wk, wv, wo, out,
     w_v, wo_v, xg, xin, xo, sc, q_s, kv, mx, rs_s, rs_r, pre, tile,
     w_sem, wol_sem, wos_sem, wor_sem, in_s, in_r, ags, agr, hs, hr, ms, mr, rss, rsr, out_s, out_r) = refs
    f32, bf16 = jnp.float32, jnp.bfloat16
    tok = ccols * WIN_R
    half = tok // 2
    sp, tp = lax.axis_index("sp"), lax.axis_index("tp")
    core, yy = lax.rem(tp, 2), lax.div(tp, 2)
    partner = yy * 2 + 1 - core
    ypeer = (1 - yy) * 2 + core
    diag = (1 - yy) * 2 + 1 - core
    right, left = lax.rem(sp + 1, n), lax.rem(sp + n - 1, n)

    def remote(src, dst, ssem, rsem, dev):
        return pltpu.make_async_remote_copy(
            src_ref=src, dst_ref=dst, send_sem=ssem, recv_sem=rsem, device_id=dev, device_id_type=MESH
        )

    bar = pltpu.get_barrier_semaphore()
    for k in range(1, n):
        pl.semaphore_signal(bar, inc=1, device_id=(lax.rem(sp + k, n), tp), device_id_type=MESH)
    pl.semaphore_signal(bar, inc=1, device_id=(sp, partner), device_id_type=MESH)
    pl.semaphore_signal(bar, inc=1, device_id=(sp, ypeer), device_id_type=MESH)
    pl.semaphore_wait(bar, n + 1)

    first = (1, 2, 3, 0)
    for i in first:
        for k in range(1, n):
            to = lax.rem(sp + k, n)
            remote(xt.at[to, i], xin.at[i, sp], in_s.at[i], in_r.at[i], (to, tp)).start()

    def weight_copies(l):
        return [pltpu.make_async_copy(w.at[l], w_v.at[l, m], w_sem.at[l, m]) for m, w in enumerate((wk, wv, wq))]

    def cols_of(c, other):
        y_of = (1 - yy) if other else yy
        return pl.ds(pl.multiple_of((y_of * 2 + c) * chan, 128), chan)

    def own_out(l):
        return [pltpu.make_async_copy(wo.at[l, :, cols_of(core, o)], wo_v.at[l, core, o], wol_sem.at[l, o]) for o in range(2)]

    def partner_out(l):
        return [
            remote(wo.at[l, :, cols_of(1 - core, o)], wo_v.at[l, core, o], wos_sem.at[l, o], wor_sem.at[l, o], (sp, partner))
            for o in range(2)
        ]

    for l in range(layers):
        for c in weight_copies(l) + own_out(l) + partner_out(l):
            c.start()

    def build(at, carry):
        l, h = lax.div(at, heads), lax.rem(at, heads)
        b = base[l, h]
        for qc in range(ccols):
            tile[l, h, qc * WIN_R : (qc + 1) * WIN_R, :] = pltpu.roll(b, WIN_R * qc, 1) if qc else b
        return carry

    lax.fori_loop(0, layers * heads, build, 0)

    a = lax.broadcasted_iota(jnp.int32, (tok, tok), 0)
    b = lax.broadcasted_iota(jnp.int32, (tok, tok), 1)
    to_cols = (lax.div(a, WIN_R) == lax.rem(b, ccols)) & (lax.rem(a, WIN_R) == lax.div(b, ccols))
    to_rows = (lax.div(b, WIN_R) == lax.rem(a, ccols)) & (lax.rem(b, WIN_R) == lax.div(a, ccols))

    def ag_copies(l, i):
        own = xg.at[l, tp, i]
        return [
            remote(own, own, ags.at[l, i, 0], agr.at[l, i, 0], (sp, ypeer)),
            remote(own, own, ags.at[l, i, 1], agr.at[l, i, 1], (sp, partner)),
        ]

    def relay_copy(l, i):
        slot = xg.at[l, ypeer, i]
        return remote(slot, slot, ags.at[l, i, 2], agr.at[l, i, 2], (sp, partner))

    def ag_send(l, i):
        for c in ag_copies(l, i):
            c.start()

    def ag_recv(l, i):
        ag_copies(l, i)[0].wait_recv()
        relay_copy(l, i).start()
        ag_copies(l, i)[1].wait_recv()
        relay_copy(l, i).wait_recv()

    def init(i):
        xin[i, sp] = xt[sp, i]
        some = xin.at[i, pl.ds(0, n - 1)]
        pltpu.make_async_copy(some, some, in_r.at[i]).wait()
        raw = xin[i].reshape(tok, chan)
        mat = jnp.where(to_cols, 1.0, 0.0).astype(bf16)
        xg[0, tp, i] = jnp.dot(mat, raw, preferred_element_type=f32).astype(bf16)
        ag_send(0, i)

    def halo_copies(l):
        return [
            remote(kv.at[l, :, 2 * chunks], kv.at[l, :, 0], hs.at[l, 0], hr.at[l, 0], (right, tp)),
            remote(kv.at[l, :, 1], kv.at[l, :, 2 * chunks + 1], hs.at[l, 1], hr.at[l, 1], (left, tp)),
        ]

    def qkv(l, i):
        ag_recv(l, i)
        total = jnp.zeros((tok, 1), f32)
        for s in range(width // chan):
            raw = xg[l, s, i].astype(f32)
            total = total + jnp.sum(raw * raw, axis=1, keepdims=True)
            sc[:, s * chan : (s + 1) * chan] = (raw * gain[l, :, s * chan : (s + 1) * chan]).astype(bf16)
        inverse = lax.rsqrt(total / width + EPS)
        x = sc[...]
        for m in range(2):
            prod = jnp.dot(x, w_v[l, m], preferred_element_type=f32) * inverse
            kv[l, m, pl.ds(1 + 2 * i, 2)] = prod.astype(bf16).reshape(2, half, chan)
        prod = jnp.dot(x, w_v[l, 2], preferred_element_type=f32) * inverse
        q_s[i] = prod.astype(bf16) * bf16(HEAD_DIM ** (-0.5))

    def mx_copy(l, i):
        slot = mx.at[l, core, i]
        return remote(slot, slot, ms.at[l, i], mr.at[l, i], (sp, partner))

    def attend(l, i):
        lane = lax.broadcasted_iota(jnp.int32, (tok, LANES), 1)
        ones = jnp.ones((2 * tok, LANES), bf16)
        for p in range(chan // LANES):
            at = slice(p * LANES, (p + 1) * LANES)
            q = q_s[i, :, at]
            key = kv[l, 0, pl.ds(2 * i, 4), :, at].reshape(2 * tok, LANES)
            val = kv[l, 1, pl.ds(2 * i, 4), :, at].reshape(2 * tok, LANES)
            val = jnp.concatenate([val, ones], axis=1)
            res = []
            for hh in range(2):
                mine = (lane >= hh * HEAD_DIM) & (lane < (hh + 1) * HEAD_DIM)
                qm = jnp.where(mine, q, jnp.zeros_like(q))
                s = lax.dot_general(qm, key, (((1,), (1,)), ((), ())), preferred_element_type=f32)
                s = s + tile[l, 2 * p + hh]
                e = jnp.exp(s - jnp.max(s, axis=1, keepdims=True)).astype(bf16)
                o = jnp.dot(e, val, preferred_element_type=f32)
                res.append(o[:, :LANES] / o[:, LANES:])
            mx[l, core, i, :, at] = jnp.where(lane < HEAD_DIM, res[0], res[1]).astype(bf16)
        mx_copy(l, i).start()

    def rs_copy(l, i):
        return remote(rs_s.at[l, i], rs_r.at[l, i], rss.at[l, i], rsr.at[l, i], (sp, ypeer))

    def project(l, i):
        mx_copy(l, i).wait_recv()
        a0, a1 = mx[l, 0, i], mx[l, 1, i]

        def part(o):
            return jnp.dot(a0, wo_v[l, 0, o], preferred_element_type=f32) + jnp.dot(
                a1, wo_v[l, 1, o], preferred_element_type=f32
            )

        rs_s[l, i] = part(1).astype(bf16)
        rs_copy(l, i).start()
        pre[i] = xg[l, tp, i].astype(f32) + part(0)

    def updated(l, i):
        rs_copy(l, i).wait_recv()
        return (pre[i] + rs_r[l, i].astype(f32)).astype(bf16)

    def finish(l, i):
        xg[l + 1, tp, i] = updated(l, i)
        ag_send(l + 1, i)

    def out_copy(i, to):
        return remote(xo.at[i, to], out.at[sp, i], out_s.at[i], out_r.at[i], (to, tp))

    def finish_last(l, i):
        mat = jnp.where(to_rows, 1.0, 0.0).astype(bf16)
        rows = jnp.dot(mat, updated(l, i), preferred_element_type=f32).astype(bf16).reshape(n, ccols, chan)
        xo[i] = rows
        for k in range(1, n):
            out_copy(i, lax.rem(sp + k, n)).start()
        out[sp, i] = xo[i, sp]

    def layer(l, carry):
        flip = lax.rem(l, 2)

        def at(i):
            return i + flip * (chunks - 1 - 2 * i)

        p = [at(i) for i in (1, 2, 3, 0)]
        order = [at(i) for i in (2, 1, 0, 3)]
        started = l > 0
        last = l == layers - 1

        def arrive(i):
            @pl.when(started)
            def _():
                finish(l - 1, i)

            @pl.when(jnp.logical_not(started))
            def _():
                init(i)

        def leave(i):
            @pl.when(last)
            def _():
                finish_last(l, i)

            @pl.when(jnp.logical_not(last))
            def _():
                finish(l, i)

        for c in weight_copies(l):
            c.wait()
        qkv(l, p[0])
        arrive(p[2])
        qkv(l, p[1])
        arrive(p[3])
        qkv(l, p[2])
        early, late = 0, 1

        @pl.when(flip == 0)
        def _():
            halo_copies(l)[0].start()

        @pl.when(flip == 1)
        def _():
            halo_copies(l)[1].start()

        attend(l, order[0])
        for c in own_out(l):
            c.wait()
        for c in partner_out(l):
            c.wait_recv()
        project(l, order[0])
        qkv(l, p[3])

        @pl.when(flip == 0)
        def _():
            halo_copies(l)[1].start()

        @pl.when(flip == 1)
        def _():
            halo_copies(l)[0].start()

        attend(l, order[1])
        project(l, order[1])
        leave(order[0])

        @pl.when(flip == 0)
        def _():
            halo_copies(l)[0].wait_recv()

        @pl.when(flip == 1)
        def _():
            halo_copies(l)[1].wait_recv()

        attend(l, order[2])
        project(l, order[2])
        leave(order[1])

        @pl.when(flip == 0)
        def _():
            halo_copies(l)[1].wait_recv()

        @pl.when(flip == 1)
        def _():
            halo_copies(l)[0].wait_recv()

        attend(l, order[3])
        project(l, order[3])
        return carry

    init(first[0])
    init(first[1])
    lax.fori_loop(0, layers, layer, 0)
    flip = (layers - 1) % 2
    for i in (0, 3):
        finish_last(layers - 1, chunks - 1 - i if flip else i)

    for i in range(chunks):
        some = out.at[pl.ds(0, n - 1), i]
        pltpu.make_async_copy(some, some, out_r.at[i]).wait()
        some = xo.at[i, pl.ds(0, n - 1)]
        pltpu.make_async_copy(some, some, out_s.at[i]).wait()
        some = xt.at[pl.ds(0, n - 1), i]
        pltpu.make_async_copy(some, some, in_s.at[i]).wait()
    for l in range(layers):
        for c in partner_out(l) + halo_copies(l):
            c.wait_send()
        for i in range(chunks):
            for c in ag_copies(l, i) + [relay_copy(l, i), mx_copy(l, i), rs_copy(l, i)]:
                c.wait_send()


def fused_body(token_grid, norm_gain, w_query, w_key, w_value, w_out, rel_bias):
    n = lax.axis_size("sp")
    rows_dev, chan, columns = token_grid.shape
    layers, width = norm_gain.shape
    heads = rel_bias.shape[1]
    chunks = columns // n // WIN_C
    bf16, f32 = jnp.bfloat16, jnp.float32
    turned = jnp.transpose(token_grid, (0, 2, 1)).reshape(n, chunks, WIN_C, chan)
    swapped = jnp.swapaxes(rel_bias, 2, 3)
    half_r = WIN_R // 2
    rows = [jnp.roll(swapped, r - half_r, axis=3).reshape(layers, heads, LANES) for r in range(WIN_R)]
    base = jnp.stack(rows, axis=2)
    base = jnp.concatenate([base, jnp.full_like(base, NEG)], axis=3)
    tok = WIN_C * WIN_R
    half = tok // 2
    cfg = (layers, n, chunks, WIN_C, chan, heads, width)
    vmem = pl.BlockSpec(memory_space=pltpu.VMEM)
    hbm = pl.BlockSpec(memory_space=pl.ANY)
    dma = pltpu.SemaphoreType.DMA
    out = pl.pallas_call(
        functools.partial(mega_kernel, cfg),
        out_shape=jax.ShapeDtypeStruct((n, chunks, WIN_C, chan), bf16),
        in_specs=[vmem, vmem, vmem, hbm, hbm, hbm, hbm],
        out_specs=vmem,
        scratch_shapes=[
            pltpu.VMEM((layers, 3, width, chan), bf16),
            pltpu.VMEM((layers, 2, 2, chan, chan), bf16),
            pltpu.VMEM((layers, width // chan, chunks, tok, chan), bf16),
            pltpu.VMEM((chunks, n, WIN_C, chan), bf16),
            pltpu.VMEM((chunks, n, WIN_C, chan), bf16),
            pltpu.VMEM((tok, width), bf16),
            pltpu.VMEM((chunks, tok, chan), bf16),
            pltpu.VMEM((layers, 2, 2 * chunks + 2, half, chan), bf16),
            pltpu.VMEM((layers, 2, chunks, tok, chan), bf16),
            pltpu.VMEM((layers, chunks, tok, chan), bf16),
            pltpu.VMEM((layers, chunks, tok, chan), bf16),
            pltpu.VMEM((chunks, tok, chan), f32),
            pltpu.VMEM((layers, heads, tok, 2 * tok), f32),
            dma((layers, 3)),
            dma((layers, 2)),
            dma((layers, 2)),
            dma((layers, 2)),
            dma((chunks,)),
            dma((chunks,)),
            dma((layers, chunks, 3)),
            dma((layers, chunks, 3)),
            dma((layers, 2)),
            dma((layers, 2)),
            dma((layers, chunks)),
            dma((layers, chunks)),
            dma((layers, chunks)),
            dma((layers, chunks)),
            dma((chunks,)),
            dma((chunks,)),
        ],
        compiler_params=pltpu.CompilerParams(
            collective_id=0, has_side_effects=True, vmem_limit_bytes=60 * 1024 * 1024
        ),
        name="grid_attention",
    )(turned, norm_gain.astype(f32).reshape(layers, 1, width), base, w_query, w_key, w_value, w_out)
    return jnp.transpose(out.reshape(rows_dev, columns, chan), (0, 2, 1))


def solution(mesh):
    in_specs = (
        P("sp", "tp", None),
        P(),
        P(None, None, "tp"),
        P(None, None, "tp"),
        P(None, None, "tp"),
        P(None, "tp", None),
        P(None, "tp", None, None),
    )
    out_specs = P("sp", "tp", None)
    sharded = functools.partial(jax.shard_map, mesh=mesh, in_specs=in_specs, out_specs=out_specs, check_vma=False)

    def run(token_grid, *rest):
        rows, _, columns = token_grid.shape
        n = mesh.shape["sp"]
        whole = rows == n == WIN_R and columns == 4 * WIN_C * n and mesh.shape["tp"] == 4
        return sharded(fused_body if whole else body)(token_grid, *rest)

    return run
```

```python
import functools

import jax
import jax.numpy as jnp
from jax import lax
from jax.experimental import pallas as pl
from jax.experimental.pallas import tpu as pltpu
from jax.sharding import PartitionSpec as P

HEAD_DIM = 64
WIN_R = 8
WIN_C = 16
EPS = 1e-06
LANES = 128
NEG = -1e30
MESH = pl.DeviceIdType.MESH


def attention_kernel(rows, cols, q_ref, k_ref, v_ref, kh_ref, vh_ref, base_ref, o_ref, tile_ref):
    pack = LANES // cols
    n_slots = min(rows, pack + WIN_R - 1)
    half_r = WIN_R // 2
    span = cols + WIN_C
    lane = lax.broadcasted_iota(jnp.int32, (8, LANES), 1)
    lane_q = lax.broadcasted_iota(jnp.int32, (LANES, LANES), 1)
    v_main = v_ref[...].T
    v_halo = vh_ref[...].T
    neg = jnp.full((8, LANES), NEG, jnp.float32)
    outs = [[] for _ in range(rows * cols // LANES)]
    for head in range(LANES // HEAD_DIM):
        for p in range(pack):
            own = (lane >= p * cols) & (lane < (p + 1) * cols)
            for slot in range(WIN_R):
                e = (slot + p) % rows
                start = jnp.broadcast_to(base_ref[head, slot : slot + 1, :], (8, LANES))
                start = pltpu.roll(start, 0, 1, stride=1, stride_axis=0)
                for blk in range(span // 8):
                    shift = (p * cols + 8 * blk) % LANES
                    moved = pltpu.roll(start, shift, 1) if shift else start
                    at = blk - 1 if 1 <= blk <= cols // 8 else (cols // 8 if blk == 0 else blk)
                    where = pl.ds(e * span + 8 * at, 8)
                    rest = neg if p == 0 and rows == WIN_R else tile_ref[where, :]
                    tile_ref[where, :] = jnp.where(own, moved, rest)
        for group in range(rows * cols // LANES):
            key_rows = [r for r in range(rows) if (r - group * pack + half_r) % rows < n_slots]
            q = q_ref[group * LANES : (group + 1) * LANES, :]
            mine = (lane_q >= head * HEAD_DIM) & (lane_q < (head + 1) * HEAD_DIM)
            q = jnp.where(mine, q, jnp.zeros_like(q))
            s_list = []
            contract = (((1,), (1,)), ((), ()))
            if len(key_rows) == rows:
                s_main = lax.dot_general(k_ref[...], q, contract, preferred_element_type=jnp.float32)
                s_halo = lax.dot_general(kh_ref[...], q, contract, preferred_element_type=jnp.float32)
            main_list = []
            halo_list = []
            for r in key_rows:
                e = (r - group * pack + half_r) % rows
                if len(key_rows) == rows:
                    main = s_main[r * cols : (r + 1) * cols]
                    halo = s_halo[r * WIN_C : (r + 1) * WIN_C]
                else:
                    main = lax.dot_general(
                        k_ref[r * cols : (r + 1) * cols, :], q, contract, preferred_element_type=jnp.float32
                    )
                    halo = lax.dot_general(
                        kh_ref[r * WIN_C : (r + 1) * WIN_C, :], q, contract, preferred_element_type=jnp.float32
                    )
                main_list.append(main + tile_ref[e * span : e * span + cols, :])
                halo_list.append(halo + tile_ref[e * span + cols : (e + 1) * span, :])
            main = jnp.concatenate(main_list, axis=0)
            halo = jnp.concatenate(halo_list, axis=0)
            top = jnp.maximum(jnp.max(main, axis=0, keepdims=True), jnp.max(halo, axis=0, keepdims=True))
            main = jnp.exp(main - top)
            halo = jnp.exp(halo - top)
            total = jnp.sum(main, axis=0, keepdims=True) + jnp.sum(halo, axis=0, keepdims=True)
            main = main.astype(jnp.bfloat16)
            halo = halo.astype(jnp.bfloat16)
            lo = head * HEAD_DIM
            if len(key_rows) == rows:
                vm = v_main[lo : lo + HEAD_DIM]
                vh = v_halo[lo : lo + HEAD_DIM]
            else:
                vm = jnp.concatenate([v_main[lo : lo + HEAD_DIM, r * cols : (r + 1) * cols] for r in key_rows], axis=1)
                vh = jnp.concatenate(
                    [v_halo[lo : lo + HEAD_DIM, r * WIN_C : (r + 1) * WIN_C] for r in key_rows], axis=1
                )
            mixed = jnp.dot(vm, main, preferred_element_type=jnp.float32)
            mixed = mixed + jnp.dot(vh, halo, preferred_element_type=jnp.float32)
            outs[group].append(mixed / total)
    for group in range(rows * cols // LANES):
        both = jnp.concatenate(outs[group], axis=0)
        o_ref[group * LANES : (group + 1) * LANES, :] = both.T.astype(o_ref.dtype)


def attention_kernel_init(rows, cols, *refs):
    tile_ref = refs[-1]
    tile_ref[...] = jnp.full(tile_ref.shape, NEG, jnp.float32)
    attention_kernel(rows, cols, *refs)


def attention(queries, keys, values, halo, base, rows, cols):
    tokens, channels = queries.shape
    n_slots = min(rows, LANES // cols + WIN_R - 1)
    pairs = channels // LANES
    per = LANES // HEAD_DIM
    side = halo.shape[0]
    kernel = attention_kernel if rows == WIN_R else attention_kernel_init
    return pl.pallas_call(
        functools.partial(kernel, rows, cols),
        grid=(pairs,),
        out_shape=jax.ShapeDtypeStruct((tokens, channels), jnp.bfloat16),
        in_specs=[
            pl.BlockSpec((tokens, LANES), lambda i: (0, i)),
            pl.BlockSpec((tokens, LANES), lambda i: (0, i)),
            pl.BlockSpec((tokens, LANES), lambda i: (0, i)),
            pl.BlockSpec((side, LANES), lambda i: (0, i)),
            pl.BlockSpec((side, LANES), lambda i: (0, i + pairs)),
            pl.BlockSpec((per, WIN_R, LANES), lambda i: (i, 0, 0)),
        ],
        out_specs=pl.BlockSpec((tokens, LANES), lambda i: (0, i)),
        scratch_shapes=[pltpu.VMEM((n_slots * (cols + WIN_C), LANES), jnp.float32)],
        compiler_params=pltpu.CompilerParams(vmem_limit_bytes=48 * 1024 * 1024),
        name="window_attention",
    )(queries, keys, values, halo, halo, base)


def body(token_grid, norm_gain, w_query, w_key, w_value, w_out, rel_bias):
    n = lax.axis_size("sp")
    rows_dev, channels, columns = token_grid.shape
    rows = rows_dev * n
    cols = columns // n
    tokens = rows * cols
    width = norm_gain.shape[1]
    factor = HEAD_DIM ** (-0.5)
    half_c = WIN_C // 2
    base = jnp.concatenate(
        [
            rel_bias[..., :1],
            jnp.full(rel_bias.shape[:-1] + (LANES - WIN_C,), NEG, jnp.float32),
            jnp.flip(rel_bias[..., 1:], axis=-1),
        ],
        axis=-1,
    )
    turned = jnp.transpose(token_grid, (2, 0, 1)).reshape(columns, rows_dev * channels)
    current = lax.all_to_all(turned, "sp", split_axis=0, concat_axis=0, tiled=True)
    to_right = [(i, (i + 1) % n) for i in range(n)]
    to_left = [(i, (i - 1) % n) for i in range(n)]
    for layer in range(norm_gain.shape[0]):
        gain = norm_gain[layer].astype(jnp.float32)
        raw = lax.all_gather(current, "tp", axis=1, tiled=True).astype(jnp.float32)
        scaled = (raw * gain[None, :]).astype(jnp.bfloat16)
        inverse = lax.rsqrt(jnp.sum(raw * raw, axis=1, keepdims=True) / width + EPS)

        def project(weight, scale=1.0):
            product = jnp.dot(scaled, weight[layer], preferred_element_type=jnp.float32)
            return (product * inverse).astype(jnp.bfloat16) * jnp.bfloat16(scale)

        keys = project(w_key)
        values = project(w_value)
        keyval = jnp.concatenate([keys, values], axis=1).reshape(rows, cols, 2 * channels)
        left = lax.ppermute(keyval[:, cols - half_c :], "sp", to_right)
        right = lax.ppermute(keyval[:, :half_c], "sp", to_left)
        queries = project(w_query, factor)
        halo = jnp.concatenate([left, right], axis=1).reshape(rows * WIN_C, 2 * channels)
        mixed = attention(queries, keys, values, halo, base[layer], rows, cols)
        partial = jnp.dot(mixed, w_out[layer], preferred_element_type=jnp.float32).astype(jnp.bfloat16)
        update = lax.psum_scatter(partial, "tp", scatter_dimension=1, tiled=True)
        current = (current.astype(jnp.float32) + update.astype(jnp.float32)).astype(jnp.bfloat16)
    back = lax.all_to_all(current, "sp", split_axis=0, concat_axis=0, tiled=True)
    return jnp.transpose(back.reshape(columns, rows_dev, channels), (1, 2, 0))

def mega_kernel(cfg, *refs):
    layers, n, chunks, ccols, chan, heads, width = cfg
    (xt, gain, bias, wq, wk, wv, wo, out,
     w_v, wo_v, xg, xin, xo, sc, q_s, kv, mx, rs_s, rs_r, pre, tile, wide,
     w_sem, wol_sem, wos_sem, wor_sem, in_s, in_r, ags, agr, hs, hr, ms, mr, rss, rsr, out_s, out_r) = refs
    f32, bf16 = jnp.float32, jnp.bfloat16
    tok = ccols * WIN_R
    half = tok // 2
    sp, tp = lax.axis_index("sp"), lax.axis_index("tp")
    core, yy = lax.rem(tp, 2), lax.div(tp, 2)
    partner = yy * 2 + 1 - core
    ypeer = (1 - yy) * 2 + core
    diag = (1 - yy) * 2 + 1 - core
    right, left = lax.rem(sp + 1, n), lax.rem(sp + n - 1, n)

    def remote(src, dst, ssem, rsem, dev):
        return pltpu.make_async_remote_copy(
            src_ref=src, dst_ref=dst, send_sem=ssem, recv_sem=rsem, device_id=dev, device_id_type=MESH
        )

    bar = pltpu.get_barrier_semaphore()
    for k in range(1, n):
        pl.semaphore_signal(bar, inc=1, device_id=(lax.rem(sp + k, n), tp), device_id_type=MESH)
    pl.semaphore_signal(bar, inc=1, device_id=(sp, partner), device_id_type=MESH)
    pl.semaphore_signal(bar, inc=1, device_id=(sp, ypeer), device_id_type=MESH)
    pl.semaphore_wait(bar, n + 1)

    first = (1, 2, 3, 0)
    for i in first:
        for k in range(1, n):
            to = lax.rem(sp + k, n)
            remote(xt.at[to, i], xin.at[i, sp], in_s.at[i], in_r.at[i], (to, tp)).start()

    def weight_copies(l):
        return [pltpu.make_async_copy(w.at[l], w_v.at[l, m], w_sem.at[l, m]) for m, w in enumerate((wk, wv, wq))]

    def cols_of(c, other):
        y_of = (1 - yy) if other else yy
        return pl.ds(pl.multiple_of((y_of * 2 + c) * chan, 128), chan)

    def own_out(l):
        return [pltpu.make_async_copy(wo.at[l, :, cols_of(core, o)], wo_v.at[l, core, o], wol_sem.at[l, o]) for o in range(2)]

    def partner_out(l):
        return [
            remote(wo.at[l, :, cols_of(1 - core, o)], wo_v.at[l, core, o], wos_sem.at[l, o], wor_sem.at[l, o], (sp, partner))
            for o in range(2)
        ]

    for l in range(layers):
        for c in weight_copies(l) + own_out(l) + partner_out(l):
            c.start()

    spread_at = lax.broadcasted_iota(jnp.int32, (ccols, LANES), 0)
    spread_to = lax.broadcasted_iota(jnp.int32, (ccols, LANES), 1)
    spread = jnp.where(lax.div(spread_to, WIN_R) == spread_at, 1.0, 0.0)
    wide[...] = jnp.dot(bias[...], spread, preferred_element_type=f32, precision=lax.Precision.HIGHEST)
    query_row = lax.broadcasted_iota(jnp.int32, (WIN_R, LANES), 0)
    key_row = lax.rem(lax.broadcasted_iota(jnp.int32, (WIN_R, LANES), 1), WIN_R)
    slot_row = lax.rem(key_row - query_row + WIN_R + WIN_R // 2, WIN_R)
    outside = jnp.full((WIN_R, LANES), NEG, f32)

    def build(at, carry):
        l, h = lax.div(at, heads), lax.rem(at, heads)
        slots = wide[pl.ds(pl.multiple_of(at * WIN_R, WIN_R), WIN_R), :]
        b = jnp.zeros((WIN_R, LANES), f32)
        for i in range(WIN_R):
            b = jnp.where(slot_row == i, slots[i : i + 1, :], b)
        b = jnp.concatenate([b, outside], axis=1)
        for qc in range(ccols):
            tile[l, h, qc * WIN_R : (qc + 1) * WIN_R, :] = pltpu.roll(b, WIN_R * qc, 1) if qc else b
        return carry

    lax.fori_loop(0, layers * heads, build, 0)

    a = lax.broadcasted_iota(jnp.int32, (tok, tok), 0)
    b = lax.broadcasted_iota(jnp.int32, (tok, tok), 1)
    to_cols = (lax.div(a, WIN_R) == lax.rem(b, ccols)) & (lax.rem(a, WIN_R) == lax.div(b, ccols))
    to_rows = (lax.div(b, WIN_R) == lax.rem(a, ccols)) & (lax.rem(b, WIN_R) == lax.div(a, ccols))

    def ag_copies(l, i):
        own = xg.at[l, tp, i]
        return [
            remote(own, own, ags.at[l, i, 0], agr.at[l, i, 0], (sp, ypeer)),
            remote(own, own, ags.at[l, i, 1], agr.at[l, i, 1], (sp, partner)),
        ]

    def relay_copy(l, i):
        slot = xg.at[l, ypeer, i]
        return remote(slot, slot, ags.at[l, i, 2], agr.at[l, i, 2], (sp, partner))

    def ag_send(l, i):
        for c in ag_copies(l, i):
            c.start()

    def ag_recv(l, i):
        ag_copies(l, i)[0].wait_recv()
        relay_copy(l, i).start()
        ag_copies(l, i)[1].wait_recv()
        relay_copy(l, i).wait_recv()

    def init(i):
        xin[i, sp] = xt[sp, i]
        some = xin.at[i, pl.ds(0, n - 1)]
        pltpu.make_async_copy(some, some, in_r.at[i]).wait()
        raw = xin[i].reshape(tok, chan)
        mat = jnp.where(to_cols, 1.0, 0.0).astype(bf16)
        xg[0, tp, i] = jnp.dot(mat, raw, preferred_element_type=f32).astype(bf16)
        ag_send(0, i)

    def halo_copies(l):
        return [
            remote(kv.at[l, :, 2 * chunks], kv.at[l, :, 0], hs.at[l, 0], hr.at[l, 0], (right, tp)),
            remote(kv.at[l, :, 1], kv.at[l, :, 2 * chunks + 1], hs.at[l, 1], hr.at[l, 1], (left, tp)),
        ]

    def qkv(l, i):
        ag_recv(l, i)
        total = jnp.zeros((tok, 1), f32)
        for s in range(width // chan):
            raw = xg[l, s, i].astype(f32)
            total = total + jnp.sum(raw * raw, axis=1, keepdims=True)
            sc[:, s * chan : (s + 1) * chan] = (raw * gain[l, :, s * chan : (s + 1) * chan]).astype(bf16)
        inverse = lax.rsqrt(total / width + EPS)
        x = sc[...]
        for m in range(2):
            prod = jnp.dot(x, w_v[l, m], preferred_element_type=f32) * inverse
            kv[l, m, pl.ds(1 + 2 * i, 2)] = prod.astype(bf16).reshape(2, half, chan)
        prod = jnp.dot(x, w_v[l, 2], preferred_element_type=f32) * inverse
        q_s[i] = prod.astype(bf16) * bf16(HEAD_DIM ** (-0.5))

    def mx_copy(l, i):
        slot = mx.at[l, core, i]
        return remote(slot, slot, ms.at[l, i], mr.at[l, i], (sp, partner))

    def attend(l, i):
        lane = lax.broadcasted_iota(jnp.int32, (tok, LANES), 1)
        ones = jnp.ones((2 * tok, LANES), bf16)
        for p in range(chan // LANES):
            at = slice(p * LANES, (p + 1) * LANES)
            q = q_s[i, :, at]
            key = kv[l, 0, pl.ds(2 * i, 4), :, at].reshape(2 * tok, LANES)
            val = kv[l, 1, pl.ds(2 * i, 4), :, at].reshape(2 * tok, LANES)
            val = jnp.concatenate([val, ones], axis=1)
            res = []
            for hh in range(2):
                mine = (lane >= hh * HEAD_DIM) & (lane < (hh + 1) * HEAD_DIM)
                qm = jnp.where(mine, q, jnp.zeros_like(q))
                s = lax.dot_general(qm, key, (((1,), (1,)), ((), ())), preferred_element_type=f32)
                s = s + tile[l, 2 * p + hh]
                e = jnp.exp(s - jnp.max(s, axis=1, keepdims=True)).astype(bf16)
                o = jnp.dot(e, val, preferred_element_type=f32)
                res.append(o[:, :LANES] / o[:, LANES:])
            mx[l, core, i, :, at] = jnp.where(lane < HEAD_DIM, res[0], res[1]).astype(bf16)
        mx_copy(l, i).start()

    def rs_copy(l, i):
        return remote(rs_s.at[l, i], rs_r.at[l, i], rss.at[l, i], rsr.at[l, i], (sp, ypeer))

    def project(l, i):
        mx_copy(l, i).wait_recv()
        a0, a1 = mx[l, 0, i], mx[l, 1, i]

        def part(o):
            return jnp.dot(a0, wo_v[l, 0, o], preferred_element_type=f32) + jnp.dot(
                a1, wo_v[l, 1, o], preferred_element_type=f32
            )

        rs_s[l, i] = part(1).astype(bf16)
        rs_copy(l, i).start()
        pre[i] = xg[l, tp, i].astype(f32) + part(0)

    def updated(l, i):
        rs_copy(l, i).wait_recv()
        return (pre[i] + rs_r[l, i].astype(f32)).astype(bf16)

    def finish(l, i):
        xg[l + 1, tp, i] = updated(l, i)
        ag_send(l + 1, i)

    def out_copy(i, to):
        return remote(xo.at[i, to], out.at[sp, i], out_s.at[i], out_r.at[i], (to, tp))

    def finish_last(l, i):
        mat = jnp.where(to_rows, 1.0, 0.0).astype(bf16)
        rows = jnp.dot(mat, updated(l, i), preferred_element_type=f32).astype(bf16).reshape(n, ccols, chan)
        xo[i] = rows
        for k in range(1, n):
            out_copy(i, lax.rem(sp + k, n)).start()
        out[sp, i] = xo[i, sp]

    def layer(l, carry):
        flip = lax.rem(l, 2)

        def at(i):
            return i + flip * (chunks - 1 - 2 * i)

        p = [at(i) for i in (1, 2, 3, 0)]
        order = [at(i) for i in (2, 1, 0, 3)]
        started = l > 0
        last = l == layers - 1

        def arrive(i):
            @pl.when(started)
            def _():
                finish(l - 1, i)

            @pl.when(jnp.logical_not(started))
            def _():
                init(i)

        def leave(i):
            @pl.when(last)
            def _():
                finish_last(l, i)

            @pl.when(jnp.logical_not(last))
            def _():
                finish(l, i)

        for c in weight_copies(l):
            c.wait()
        qkv(l, p[0])
        arrive(p[2])
        qkv(l, p[1])
        arrive(p[3])
        qkv(l, p[2])

        @pl.when(flip == 0)
        def _():
            halo_copies(l)[0].start()

        @pl.when(flip == 1)
        def _():
            halo_copies(l)[1].start()

        attend(l, order[0])
        for c in own_out(l):
            c.wait()
        for c in partner_out(l):
            c.wait_recv()
        project(l, order[0])
        qkv(l, p[3])

        @pl.when(flip == 0)
        def _():
            halo_copies(l)[1].start()

        @pl.when(flip == 1)
        def _():
            halo_copies(l)[0].start()

        attend(l, order[1])
        project(l, order[1])
        leave(order[0])

        @pl.when(flip == 0)
        def _():
            halo_copies(l)[0].wait_recv()

        @pl.when(flip == 1)
        def _():
            halo_copies(l)[1].wait_recv()

        attend(l, order[2])
        project(l, order[2])
        leave(order[1])

        @pl.when(flip == 0)
        def _():
            halo_copies(l)[1].wait_recv()

        @pl.when(flip == 1)
        def _():
            halo_copies(l)[0].wait_recv()

        attend(l, order[3])
        project(l, order[3])
        return carry

    init(first[0])
    init(first[1])
    lax.fori_loop(0, layers, layer, 0)
    flip = (layers - 1) % 2
    for i in (0, 3):
        finish_last(layers - 1, chunks - 1 - i if flip else i)

    for i in range(chunks):
        some = out.at[pl.ds(0, n - 1), i]
        pltpu.make_async_copy(some, some, out_r.at[i]).wait()
        some = xo.at[i, pl.ds(0, n - 1)]
        pltpu.make_async_copy(some, some, out_s.at[i]).wait()
        some = xt.at[pl.ds(0, n - 1), i]
        pltpu.make_async_copy(some, some, in_s.at[i]).wait()
    for l in range(layers):
        for c in partner_out(l) + halo_copies(l):
            c.wait_send()
        for i in range(chunks):
            for c in ag_copies(l, i) + [relay_copy(l, i), mx_copy(l, i), rs_copy(l, i)]:
                c.wait_send()


def fused_body(token_grid, norm_gain, w_query, w_key, w_value, w_out, rel_bias):
    n = lax.axis_size("sp")
    rows_dev, chan, columns = token_grid.shape
    layers, width = norm_gain.shape
    heads = rel_bias.shape[1]
    chunks = columns // n // WIN_C
    bf16, f32 = jnp.bfloat16, jnp.float32
    turned = jnp.transpose(token_grid, (0, 2, 1)).reshape(n, chunks, WIN_C, chan)
    tok = WIN_C * WIN_R
    half = tok // 2
    cfg = (layers, n, chunks, WIN_C, chan, heads, width)
    vmem = pl.BlockSpec(memory_space=pltpu.VMEM)
    hbm = pl.BlockSpec(memory_space=pl.ANY)
    dma = pltpu.SemaphoreType.DMA
    out = pl.pallas_call(
        functools.partial(mega_kernel, cfg),
        out_shape=jax.ShapeDtypeStruct((n, chunks, WIN_C, chan), bf16),
        in_specs=[vmem, vmem, vmem, hbm, hbm, hbm, hbm],
        out_specs=vmem,
        scratch_shapes=[
            pltpu.VMEM((layers, 3, width, chan), bf16),
            pltpu.VMEM((layers, 2, 2, chan, chan), bf16),
            pltpu.VMEM((layers, width // chan, chunks, tok, chan), bf16),
            pltpu.VMEM((chunks, n, WIN_C, chan), bf16),
            pltpu.VMEM((chunks, n, WIN_C, chan), bf16),
            pltpu.VMEM((tok, width), bf16),
            pltpu.VMEM((chunks, tok, chan), bf16),
            pltpu.VMEM((layers, 2, 2 * chunks + 2, half, chan), bf16),
            pltpu.VMEM((layers, 2, chunks, tok, chan), bf16),
            pltpu.VMEM((layers, chunks, tok, chan), bf16),
            pltpu.VMEM((layers, chunks, tok, chan), bf16),
            pltpu.VMEM((chunks, tok, chan), f32),
            pltpu.VMEM((layers, heads, tok, 2 * tok), f32),
            pltpu.VMEM((layers * heads * WIN_R, LANES), f32),
            dma((layers, 3)),
            dma((layers, 2)),
            dma((layers, 2)),
            dma((layers, 2)),
            dma((chunks,)),
            dma((chunks,)),
            dma((layers, chunks, 3)),
            dma((layers, chunks, 3)),
            dma((layers, 2)),
            dma((layers, 2)),
            dma((layers, chunks)),
            dma((layers, chunks)),
            dma((layers, chunks)),
            dma((layers, chunks)),
            dma((chunks,)),
            dma((chunks,)),
        ],
        compiler_params=pltpu.CompilerParams(
            collective_id=0, has_side_effects=True, vmem_limit_bytes=60 * 1024 * 1024
        ),
        name="grid_attention",
    )(turned, norm_gain.astype(f32).reshape(layers, 1, width), rel_bias.reshape(-1, WIN_C), w_query, w_key, w_value, w_out)
    return jnp.transpose(out.reshape(rows_dev, columns, chan), (0, 2, 1))


def solution(mesh):
    in_specs = (
        P("sp", "tp", None),
        P(),
        P(None, None, "tp"),
        P(None, None, "tp"),
        P(None, None, "tp"),
        P(None, "tp", None),
        P(None, "tp", None, None),
    )
    out_specs = P("sp", "tp", None)
    sharded = functools.partial(jax.shard_map, mesh=mesh, in_specs=in_specs, out_specs=out_specs, check_vma=False)

    def run(token_grid, *rest):
        rows, _, columns = token_grid.shape
        n = mesh.shape["sp"]
        whole = rows == n == WIN_R and columns == 4 * WIN_C * n and mesh.shape["tp"] == 4
        return sharded(fused_body if whole else body)(token_grid, *rest)

    return run
```

```python
import functools

import jax
import jax.numpy as jnp
from jax import lax
from jax.experimental import pallas as pl
from jax.experimental.pallas import tpu as pltpu
from jax.sharding import PartitionSpec as P

HEAD_DIM = 64
WIN_R = 8
WIN_C = 16
EPS = 1e-06
LANES = 128
NEG = -1e30
MESH = pl.DeviceIdType.MESH


def attention_kernel(rows, cols, q_ref, k_ref, v_ref, kh_ref, vh_ref, base_ref, o_ref, tile_ref):
    pack = LANES // cols
    n_slots = min(rows, pack + WIN_R - 1)
    half_r = WIN_R // 2
    span = cols + WIN_C
    lane = lax.broadcasted_iota(jnp.int32, (8, LANES), 1)
    lane_q = lax.broadcasted_iota(jnp.int32, (LANES, LANES), 1)
    v_main = v_ref[...].T
    v_halo = vh_ref[...].T
    neg = jnp.full((8, LANES), NEG, jnp.float32)
    outs = [[] for _ in range(rows * cols // LANES)]
    for head in range(LANES // HEAD_DIM):
        for p in range(pack):
            own = (lane >= p * cols) & (lane < (p + 1) * cols)
            for slot in range(WIN_R):
                e = (slot + p) % rows
                start = jnp.broadcast_to(base_ref[head, slot : slot + 1, :], (8, LANES))
                start = pltpu.roll(start, 0, 1, stride=1, stride_axis=0)
                for blk in range(span // 8):
                    shift = (p * cols + 8 * blk) % LANES
                    moved = pltpu.roll(start, shift, 1) if shift else start
                    at = blk - 1 if 1 <= blk <= cols // 8 else (cols // 8 if blk == 0 else blk)
                    where = pl.ds(e * span + 8 * at, 8)
                    rest = neg if p == 0 and rows == WIN_R else tile_ref[where, :]
                    tile_ref[where, :] = jnp.where(own, moved, rest)
        for group in range(rows * cols // LANES):
            key_rows = [r for r in range(rows) if (r - group * pack + half_r) % rows < n_slots]
            q = q_ref[group * LANES : (group + 1) * LANES, :]
            mine = (lane_q >= head * HEAD_DIM) & (lane_q < (head + 1) * HEAD_DIM)
            q = jnp.where(mine, q, jnp.zeros_like(q))
            s_list = []
            contract = (((1,), (1,)), ((), ()))
            if len(key_rows) == rows:
                s_main = lax.dot_general(k_ref[...], q, contract, preferred_element_type=jnp.float32)
                s_halo = lax.dot_general(kh_ref[...], q, contract, preferred_element_type=jnp.float32)
            main_list = []
            halo_list = []
            for r in key_rows:
                e = (r - group * pack + half_r) % rows
                if len(key_rows) == rows:
                    main = s_main[r * cols : (r + 1) * cols]
                    halo = s_halo[r * WIN_C : (r + 1) * WIN_C]
                else:
                    main = lax.dot_general(
                        k_ref[r * cols : (r + 1) * cols, :], q, contract, preferred_element_type=jnp.float32
                    )
                    halo = lax.dot_general(
                        kh_ref[r * WIN_C : (r + 1) * WIN_C, :], q, contract, preferred_element_type=jnp.float32
                    )
                main_list.append(main + tile_ref[e * span : e * span + cols, :])
                halo_list.append(halo + tile_ref[e * span + cols : (e + 1) * span, :])
            main = jnp.concatenate(main_list, axis=0)
            halo = jnp.concatenate(halo_list, axis=0)
            top = jnp.maximum(jnp.max(main, axis=0, keepdims=True), jnp.max(halo, axis=0, keepdims=True))
            main = jnp.exp(main - top)
            halo = jnp.exp(halo - top)
            total = jnp.sum(main, axis=0, keepdims=True) + jnp.sum(halo, axis=0, keepdims=True)
            main = main.astype(jnp.bfloat16)
            halo = halo.astype(jnp.bfloat16)
            lo = head * HEAD_DIM
            if len(key_rows) == rows:
                vm = v_main[lo : lo + HEAD_DIM]
                vh = v_halo[lo : lo + HEAD_DIM]
            else:
                vm = jnp.concatenate([v_main[lo : lo + HEAD_DIM, r * cols : (r + 1) * cols] for r in key_rows], axis=1)
                vh = jnp.concatenate(
                    [v_halo[lo : lo + HEAD_DIM, r * WIN_C : (r + 1) * WIN_C] for r in key_rows], axis=1
                )
            mixed = jnp.dot(vm, main, preferred_element_type=jnp.float32)
            mixed = mixed + jnp.dot(vh, halo, preferred_element_type=jnp.float32)
            outs[group].append(mixed / total)
    for group in range(rows * cols // LANES):
        both = jnp.concatenate(outs[group], axis=0)
        o_ref[group * LANES : (group + 1) * LANES, :] = both.T.astype(o_ref.dtype)


def attention_kernel_init(rows, cols, *refs):
    tile_ref = refs[-1]
    tile_ref[...] = jnp.full(tile_ref.shape, NEG, jnp.float32)
    attention_kernel(rows, cols, *refs)


def attention(queries, keys, values, halo, base, rows, cols):
    tokens, channels = queries.shape
    n_slots = min(rows, LANES // cols + WIN_R - 1)
    pairs = channels // LANES
    per = LANES // HEAD_DIM
    side = halo.shape[0]
    kernel = attention_kernel if rows == WIN_R else attention_kernel_init
    return pl.pallas_call(
        functools.partial(kernel, rows, cols),
        grid=(pairs,),
        out_shape=jax.ShapeDtypeStruct((tokens, channels), jnp.bfloat16),
        in_specs=[
            pl.BlockSpec((tokens, LANES), lambda i: (0, i)),
            pl.BlockSpec((tokens, LANES), lambda i: (0, i)),
            pl.BlockSpec((tokens, LANES), lambda i: (0, i)),
            pl.BlockSpec((side, LANES), lambda i: (0, i)),
            pl.BlockSpec((side, LANES), lambda i: (0, i + pairs)),
            pl.BlockSpec((per, WIN_R, LANES), lambda i: (i, 0, 0)),
        ],
        out_specs=pl.BlockSpec((tokens, LANES), lambda i: (0, i)),
        scratch_shapes=[pltpu.VMEM((n_slots * (cols + WIN_C), LANES), jnp.float32)],
        compiler_params=pltpu.CompilerParams(vmem_limit_bytes=48 * 1024 * 1024),
        name="window_attention",
    )(queries, keys, values, halo, halo, base)


def body(token_grid, norm_gain, w_query, w_key, w_value, w_out, rel_bias):
    n = lax.axis_size("sp")
    rows_dev, channels, columns = token_grid.shape
    rows = rows_dev * n
    cols = columns // n
    tokens = rows * cols
    width = norm_gain.shape[1]
    factor = HEAD_DIM ** (-0.5)
    half_c = WIN_C // 2
    base = jnp.concatenate(
        [
            rel_bias[..., :1],
            jnp.full(rel_bias.shape[:-1] + (LANES - WIN_C,), NEG, jnp.float32),
            jnp.flip(rel_bias[..., 1:], axis=-1),
        ],
        axis=-1,
    )
    turned = jnp.transpose(token_grid, (2, 0, 1)).reshape(columns, rows_dev * channels)
    current = lax.all_to_all(turned, "sp", split_axis=0, concat_axis=0, tiled=True)
    to_right = [(i, (i + 1) % n) for i in range(n)]
    to_left = [(i, (i - 1) % n) for i in range(n)]
    for layer in range(norm_gain.shape[0]):
        gain = norm_gain[layer].astype(jnp.float32)
        raw = lax.all_gather(current, "tp", axis=1, tiled=True).astype(jnp.float32)
        scaled = (raw * gain[None, :]).astype(jnp.bfloat16)
        inverse = lax.rsqrt(jnp.sum(raw * raw, axis=1, keepdims=True) / width + EPS)

        def project(weight, scale=1.0):
            product = jnp.dot(scaled, weight[layer], preferred_element_type=jnp.float32)
            return (product * inverse).astype(jnp.bfloat16) * jnp.bfloat16(scale)

        keys = project(w_key)
        values = project(w_value)
        keyval = jnp.concatenate([keys, values], axis=1).reshape(rows, cols, 2 * channels)
        left = lax.ppermute(keyval[:, cols - half_c :], "sp", to_right)
        right = lax.ppermute(keyval[:, :half_c], "sp", to_left)
        queries = project(w_query, factor)
        halo = jnp.concatenate([left, right], axis=1).reshape(rows * WIN_C, 2 * channels)
        mixed = attention(queries, keys, values, halo, base[layer], rows, cols)
        partial = jnp.dot(mixed, w_out[layer], preferred_element_type=jnp.float32).astype(jnp.bfloat16)
        update = lax.psum_scatter(partial, "tp", scatter_dimension=1, tiled=True)
        current = (current.astype(jnp.float32) + update.astype(jnp.float32)).astype(jnp.bfloat16)
    back = lax.all_to_all(current, "sp", split_axis=0, concat_axis=0, tiled=True)
    return jnp.transpose(back.reshape(columns, rows_dev, channels), (1, 2, 0))

def unit_pairs(blocks):
    odd = [(b, (b + 1) % blocks) for b in range(1, blocks, 2)]
    even = [((b + 1) % blocks, (b + 2) % blocks) for b in range(1, blocks, 2)]
    return odd, even


def plan(layers, blocks, starts, orders):
    link, hop, near, mixed, halo_link, halo_hop = 2.82, 1.8, 1.45, 1.4, 2.8, 2.2
    odd, even = unit_pairs(blocks)
    units = [odd if l % 2 == 0 else even for l in range(layers + 1)]
    count = len(odd)
    gathered = [starts] + orders

    def needs(l, i):
        wanted, sides = set(), []
        for b in units[l + 1][i]:
            for near_b in (b - 1, b, b + 1):
                if 0 <= near_b < blocks:
                    wanted.update(u for u, pair in enumerate(units[l]) if near_b in pair)
                else:
                    sides.append(near_b < 0)
        return wanted, sides

    now, wire = 0.0, 0.0
    side_wire = {True: 0.0, False: 0.0}
    own, across, relayed, done, halo, mx, sums = {}, {}, {}, set(), {}, {}, {}
    at = {kind: [0] * layers for kind in ("qkv", "attend", "project", "finish", "relay")}
    first, steps = 0, []

    def send(t, loads=1):
        nonlocal wire
        wire = max(t, wire) + loads * link
        return wire + hop

    while True:
        ready = []
        if first < count:
            ready.append((4.5 + 2.7 * first, 0, "init", 0, starts[first]))
        for l in range(layers):
            def step(kind, order):
                return order[at[kind][l]] if at[kind][l] < count else None

            i = step("finish", orders[l])
            if (l, i) in sums:
                ready.append((sums[l, i], 1, "finish", l, i))
            i = step("relay", gathered[l])
            if l == 0 and (l, i) in across:
                ready.append((across[l, i], 2, "relay", l, i))
            i = step("project", orders[l])
            if (l, i) in mx:
                ready.append((mx[l, i], 3, "project", l, i))
            i = step("attend", orders[l])
            if i is not None:
                wanted, sides = needs(l, i)
                if all((l, u) in done for u in wanted) and all((l, side) in halo for side in sides):
                    ready.append((max([0.0] + [halo[l, side] for side in sides]), 4, "attend", l, i))
            i = step("qkv", gathered[l])
            if (l, i) in relayed:
                ready.append((max(relayed[l, i], own[l, i]), 5, "qkv", l, i))
        if not ready:
            return steps
        can = [r for r in ready if r[0] <= now]
        when, _, kind, l, i = min(can, key=lambda r: r[1:]) if can else min(ready)
        now = max(now, when)
        steps.append((kind, l, i))
        if kind == "init":
            first += 1
            now += 0.18
            across[0, i], own[0, i] = send(now), now + near
            continue
        at[kind][l] += 1
        if kind == "relay":
            relayed[l, i] = now + near
        elif kind == "qkv":
            done.add((l, i))
            for side, edge in ((True, blocks - 1), (False, 0)):
                if edge in units[l][i]:
                    side_wire[side] = max(now + 0.75, side_wire[side]) + halo_link
                    halo[l, side] = side_wire[side] + halo_hop
            now += 1.02
        elif kind == "attend":
            pair = units[l + 1][i]
            now += 0.64 if pair[0] < pair[1] else 1.0
            mx[l, i] = now + mixed
        elif kind == "project":
            sums[l, i] = send(now + 0.35, 1 if l == layers - 1 else 2)
            now += 0.65
        else:
            now += 0.15
            if l < layers - 1:
                relayed[l + 1, i] = own[l + 1, i] = now + near


def mega_kernel(cfg, *refs):
    layers, n, chunks, ccols, chan, heads, width, steps = cfg
    (xt, gain, bias, wq, wk, wv, wo, out,
     w_v, wo_v, xg, xin, xo, sc, q_s, kv, mx, rs_s, rs_r, pre, tile, wide,
     w_sem, wol_sem, wos_sem, wor_sem, in_s, in_r, ags, agr, hs, hr, ms, mr, rss, rsr, out_s, out_r) = refs
    f32, bf16 = jnp.float32, jnp.bfloat16
    tok = ccols * WIN_R
    half = tok // 2
    sp, tp = lax.axis_index("sp"), lax.axis_index("tp")
    core, yy = lax.rem(tp, 2), lax.div(tp, 2)
    partner = yy * 2 + 1 - core
    ypeer = (1 - yy) * 2 + core
    diag = (1 - yy) * 2 + 1 - core
    deep = n // 2

    def place(dev):
        z, x = lax.div(dev, 2), lax.rem(dev, 2)
        return z + x * (n - 1 - 2 * z)

    def holder(at):
        back = lax.div(at, deep)
        return 2 * (at + back * (n - 1 - 2 * at)) + back

    mine_at = place(sp)
    right, left = holder(lax.rem(mine_at + 1, n)), holder(lax.rem(mine_at + n - 1, n))

    def remote(src, dst, ssem, rsem, dev):
        return pltpu.make_async_remote_copy(
            src_ref=src, dst_ref=dst, send_sem=ssem, recv_sem=rsem, device_id=dev, device_id_type=MESH
        )

    bar = pltpu.get_barrier_semaphore()
    for k in range(1, n):
        pl.semaphore_signal(bar, inc=1, device_id=(lax.rem(sp + k, n), tp), device_id_type=MESH)
    pl.semaphore_signal(bar, inc=1, device_id=(sp, partner), device_id_type=MESH)
    pl.semaphore_signal(bar, inc=1, device_id=(sp, ypeer), device_id_type=MESH)
    pl.semaphore_wait(bar, n + 1)

    blocks = 2 * chunks
    odd, even = unit_pairs(blocks)
    units = [odd if l % 2 == 0 else even for l in range(layers + 1)]

    def sends_in(i):
        (b0, b1), out = odd[i], []
        for k in range(1, n):
            to = lax.rem(sp + k, n)
            if b1 == b0 + 1:
                out.append(remote(xt.at[place(to), b0 : b0 + 2], xin.at[i, :, sp], in_s.at[i], in_r.at[i], (to, tp)))
            else:
                for j, blk in enumerate((b0, b1)):
                    out.append(remote(xt.at[place(to), blk], xin.at[i, j, sp], in_s.at[i], in_r.at[i], (to, tp)))
        return out

    def sent_in(i):
        some = xin.at[i, :, pl.ds(0, n - 1)]
        pltpu.make_async_copy(some, some, in_s.at[i]).wait()

    for i in range(2):
        for c in sends_in(i):
            c.start()

    def weight_copies(l):
        return [pltpu.make_async_copy(w.at[l], w_v.at[l, m], w_sem.at[l, m]) for m, w in enumerate((wk, wv, wq))]

    def cols_of(c, o):
        return pl.ds(pl.multiple_of((o * 2 + c) * chan, 128), chan)

    def own_out(l):
        return [pltpu.make_async_copy(wo.at[l, :, cols_of(core, o)], wo_v.at[l, core, o], wol_sem.at[l, o]) for o in range(2)]

    def partner_out(l):
        return [
            remote(wo.at[l, :, cols_of(1 - core, o)], wo_v.at[l, core, o], wos_sem.at[l, o], wor_sem.at[l, o], (sp, partner))
            for o in range(2)
        ]

    for c in weight_copies(0) + own_out(0) + partner_out(0):
        c.start()

    spread_at = lax.broadcasted_iota(jnp.int32, (ccols, LANES), 0)
    spread_to = lax.broadcasted_iota(jnp.int32, (ccols, LANES), 1)
    spread = jnp.where(lax.div(spread_to, WIN_R) == spread_at, 1.0, 0.0)
    wide[...] = jnp.dot(bias[...], spread, preferred_element_type=f32, precision=lax.Precision.HIGHEST)
    query_row = lax.broadcasted_iota(jnp.int32, (WIN_R, LANES), 0)
    key_row = lax.rem(lax.broadcasted_iota(jnp.int32, (WIN_R, LANES), 1), WIN_R)
    slot_row = lax.rem(key_row - query_row + WIN_R + WIN_R // 2, WIN_R)
    outside = jnp.full((WIN_R, LANES), NEG, f32)

    def build(at, carry):
        l, h = lax.div(at, heads), lax.rem(at, heads)
        slots = wide[pl.ds(pl.multiple_of(at * WIN_R, WIN_R), WIN_R), :]
        b = jnp.zeros((WIN_R, LANES), f32)
        for i in range(WIN_R):
            b = jnp.where(slot_row == i, slots[i : i + 1, :], b)
        b = jnp.concatenate([b, outside], axis=1)
        for qc in range(ccols):
            tile[l, h, qc * WIN_R : (qc + 1) * WIN_R, :] = pltpu.roll(b, WIN_R * qc, 1) if qc else b
        return carry

    lax.fori_loop(0, layers * heads, build, 0)

    for i in range(2, chunks):
        sent_in(i - 2)
        for c in sends_in(i):
            c.start()

    a = lax.broadcasted_iota(jnp.int32, (tok, tok), 0)
    b = lax.broadcasted_iota(jnp.int32, (tok, tok), 1)
    same = lax.div(a, half) == lax.div(b, half)
    ra, rb = lax.rem(a, half), lax.rem(b, half)
    swap = same & (lax.div(ra, WIN_R) == lax.rem(rb, WIN_R)) & (lax.rem(ra, WIN_R) == lax.div(rb, WIN_R))
    swap = jnp.where(swap, 1.0, 0.0).astype(bf16)

    def ag_copies(l, i):
        own = xg.at[l, tp, i]
        return [
            remote(own, own, ags.at[l, i, 0], agr.at[l, i, 0], (sp, ypeer)),
            remote(own, own, ags.at[l, i, 1], agr.at[l, i, 1], (sp, partner)),
        ]

    def relay_copy(l, i):
        slot = xg.at[l, ypeer, i]
        return remote(slot, slot, ags.at[l, i, 2], agr.at[l, i, 2], (sp, partner))

    def ag_send(l, i):
        for c in ag_copies(l, i):
            c.start()

    def relay(l, i):
        ag_copies(l, i)[0].wait_recv()
        relay_copy(l, i).start()

    def partner_copies(l, i):
        slots = [xg.at[l, 2 * o + core, i] for o in range(2)]
        return [remote(slots[o], slots[o], ags.at[l, i, o], agr.at[l, i, o], (sp, partner)) for o in range(2)]

    def ag_recv(l, i):
        if l == 0:
            ag_copies(l, i)[1].wait_recv()
            relay_copy(l, i).wait_recv()
        else:
            for c in partner_copies(l, i):
                c.wait_recv()

    def init(i):
        b0, b1 = odd[i]
        for j, blk in enumerate((b0, b1)):
            xin[i, j, sp] = xt[mine_at, blk]
        some = xin.at[i, :, pl.ds(0, n - 1)]
        pltpu.make_async_copy(some, some, in_r.at[i]).wait()
        raw = xin[i].astype(f32).reshape(tok, chan).astype(bf16)
        xg[0, tp, i] = jnp.dot(swap, raw, preferred_element_type=f32).astype(bf16)
        ag_send(0, i)

    def halo_copies(l):
        return [
            remote(kv.at[l, :, 2 * chunks], kv.at[l, :, 0], hs.at[l, 0], hr.at[l, 0], (right, tp)),
            remote(kv.at[l, :, 1], kv.at[l, :, 2 * chunks + 1], hs.at[l, 1], hr.at[l, 1], (left, tp)),
        ]

    def qkv(l, i):
        ag_recv(l, i)
        total = jnp.zeros((tok, 1), f32)
        for s in range(width // chan):
            raw = xg[l, s, i].astype(f32)
            total = total + jnp.sum(raw * raw, axis=1, keepdims=True)
            sc[:, s * chan : (s + 1) * chan] = (raw * gain[l, :, s * chan : (s + 1) * chan]).astype(bf16)
        inverse = lax.rsqrt(total / width + EPS)
        x = sc[...]
        for m in range(2):
            prod = jnp.dot(x, w_v[l, m], preferred_element_type=f32) * inverse
            prod = prod.astype(bf16)
            for j, blk in enumerate(units[l][i]):
                kv[l, m, 1 + blk] = prod[j * half : (j + 1) * half]
        if 0 in units[l][i]:
            halo_copies(l)[1].start()
        if blocks - 1 in units[l][i]:
            halo_copies(l)[0].start()
        prod = jnp.dot(x, w_v[l, 2], preferred_element_type=f32) * inverse
        prod = prod.astype(bf16) * bf16(HEAD_DIM ** (-0.5))
        for j, blk in enumerate(units[l][i]):
            q_s[blk] = prod[j * half : (j + 1) * half]

    def mx_copy(l, i):
        slot = mx.at[l, core, i]
        return remote(slot, slot, ms.at[l, i], mr.at[l, i], (sp, partner))

    def window(l, q0, qn, k0, t0, out_at):
        rows = qn * half
        lane = lax.broadcasted_iota(jnp.int32, (rows, LANES), 1)
        ones = jnp.ones((2 * tok, LANES), bf16)
        for p in range(chan // LANES):
            at = slice(p * LANES, (p + 1) * LANES)
            q = q_s[q0 : q0 + qn, :, at].reshape(rows, LANES)
            key = kv[l, 0, k0 : k0 + 4, :, at].reshape(2 * tok, LANES)
            val = kv[l, 1, k0 : k0 + 4, :, at].reshape(2 * tok, LANES)
            val = jnp.concatenate([val, ones], axis=1)
            res = []
            for hh in range(2):
                mine = (lane >= hh * HEAD_DIM) & (lane < (hh + 1) * HEAD_DIM)
                qm = jnp.where(mine, q, jnp.zeros_like(q))
                s = lax.dot_general(qm, key, (((1,), (1,)), ((), ())), preferred_element_type=f32)
                s = s + tile[l, 2 * p + hh, t0 : t0 + rows]
                e = jnp.exp(s - jnp.max(s, axis=1, keepdims=True)).astype(bf16)
                o = jnp.dot(e, val, preferred_element_type=f32)
                res.append(o[:, :LANES] / o[:, LANES:])
            out_at[:, at] = jnp.where(lane < HEAD_DIM, res[0], res[1]).astype(bf16)

    def attend(l, i):
        b0, b1 = units[l + 1][i]
        if b1 == b0 + 1:
            window(l, b0, 2, b0, 0, mx.at[l, core, i])
        else:
            window(l, b0, 1, b0 - 1, half, mx.at[l, core, i, :half])
            window(l, b1, 1, b1, 0, mx.at[l, core, i, half:])
        mx_copy(l, i).start()

    def rs_copy(l, i, o):
        return remote(rs_s.at[l, i, o], rs_r.at[l, i, o], rss.at[l, i, o], rsr.at[l, i, o], (sp, ypeer))

    def old(l, i, slot):
        parts = []
        for blk in units[l + 1][i]:
            u = [blk in pair for pair in units[l]].index(True)
            k = units[l][u].index(blk)
            parts.append(xg[l, slot, u, k * half : (k + 1) * half])
        return jnp.concatenate(parts, axis=0).astype(f32)

    def project(l, i):
        mx_copy(l, i).wait_recv()
        a0, a1 = mx[l, 0, i], mx[l, 1, i]

        def part(o):
            return jnp.dot(a0, wo_v[l, 0, o], preferred_element_type=f32) + jnp.dot(
                a1, wo_v[l, 1, o], preferred_element_type=f32
            )

        if l == layers - 1:
            rs_s[l, i, 0] = part(1 - yy).astype(bf16)
            rs_copy(l, i, 0).start()
            pre[i] = old(l, i, tp) + part(yy)
        else:
            for o in range(2):
                rs_s[l, i, o] = part(o).astype(bf16)
                rs_copy(l, i, o).start()

    def updated(i):
        rs_copy(layers - 1, i, 0).wait_recv()
        return (pre[i] + rs_r[layers - 1, i, 0].astype(f32)).astype(bf16)

    def finish(l, i):
        for o in range(2):
            rs_copy(l, i, o).wait_recv()
            slot = 2 * o + core
            both = rs_s[l, i, o].astype(f32) + rs_r[l, i, o].astype(f32)
            xg[l + 1, slot, i] = (old(l, i, slot) + both).astype(bf16)
            partner_copies(l + 1, i)[o].start()

    def out_copies(i):
        (b0, b1), out_list = units[layers][i], []
        for k in range(1, n):
            to = lax.rem(sp + k, n)
            if b1 == b0 + 1:
                out_list.append(remote(xo.at[i, :, to], out.at[mine_at, b0 : b0 + 2], out_s.at[i], out_r.at[i], (to, tp)))
            else:
                for j, blk in enumerate((b0, b1)):
                    out_list.append(remote(xo.at[i, j, to], out.at[mine_at, blk], out_s.at[i], out_r.at[i], (to, tp)))
        return out_list

    def finish_last(i):
        rows = jnp.dot(swap, updated(i), preferred_element_type=f32)
        xo[i] = rows.reshape(2, n, half // n, chan).astype(bf16)
        for c in out_copies(i):
            c.start()
        for j, blk in enumerate(units[layers][i]):
            out[mine_at, blk] = xo[i, j, sp]

    def leave(l, i):
        if l == layers - 1:
            finish_last(i)
        else:
            finish(l, i)

    def load(l, what):
        for c in what(l):
            c.start()

    seen = set()

    def once(*key):
        fresh = key not in seen
        seen.add(key)
        return fresh

    for kind, l, i in steps:
        if kind == "init":
            init(i)
            if l + 1 < layers and once("load", l + 1):
                load(l + 1, weight_copies)
                load(l + 1, own_out)
        elif kind == "relay":
            relay(l, i)
        elif kind == "qkv":
            if once("weights", l):
                for c in weight_copies(l):
                    c.wait()
            qkv(l, i)
        elif kind == "attend":
            for blk in units[l + 1][i]:
                if blk in (0, blocks - 1) and once("halo", l, blk):
                    halo_copies(l)[0 if blk == 0 else 1].wait_recv()
            attend(l, i)
        elif kind == "project":
            if once("out", l):
                for c in own_out(l):
                    c.wait()
                for c in partner_out(l):
                    c.wait_recv()
            project(l, i)
            if l + 1 < layers and once("load out", l + 1):
                load(l + 1, partner_out)
            if l + 2 < layers and once("load", l + 2):
                load(l + 2, weight_copies)
                load(l + 2, own_out)
        else:
            leave(l, i)

    for i in range(chunks):
        some = xo.at[i, :, pl.ds(0, n - 1)]
        pltpu.make_async_copy(some, some, out_r.at[i]).wait()
        pltpu.make_async_copy(some, some, out_s.at[i]).wait()
        if i >= chunks - 2:
            sent_in(i)
    for l in range(layers):
        for c in partner_out(l) + halo_copies(l):
            c.wait_send()
        for i in range(chunks):
            moved = ag_copies(l, i) + [relay_copy(l, i)] if l == 0 else partner_copies(l, i)
            moved += [mx_copy(l, i)] + [rs_copy(l, i, o) for o in range(1 if l == layers - 1 else 2)]
            for c in moved:
                c.wait_send()


def fused_body(token_grid, norm_gain, w_query, w_key, w_value, w_out, rel_bias):
    n = lax.axis_size("sp")
    rows_dev, chan, columns = token_grid.shape
    layers, width = norm_gain.shape
    heads = rel_bias.shape[1]
    chunks = columns // n // WIN_C
    bf16, f32 = jnp.bfloat16, jnp.float32
    turned = jnp.transpose(token_grid, (0, 2, 1)).reshape(n, 2 * chunks, WIN_C // 2, chan)
    tok = WIN_C * WIN_R
    half = tok // 2
    same = tuple(range(chunks))
    orders = [same[:-2] + (same[-1], same[-2])] * (layers - 1) + [same]
    cfg = (layers, n, chunks, WIN_C, chan, heads, width, plan(layers, 2 * chunks, same, orders))
    vmem = pl.BlockSpec(memory_space=pltpu.VMEM)
    hbm = pl.BlockSpec(memory_space=pl.ANY)
    dma = pltpu.SemaphoreType.DMA
    out = pl.pallas_call(
        functools.partial(mega_kernel, cfg),
        out_shape=jax.ShapeDtypeStruct((n, 2 * chunks, WIN_C // 2, chan), bf16),
        in_specs=[vmem, vmem, vmem, hbm, hbm, hbm, hbm],
        out_specs=vmem,
        scratch_shapes=[
            pltpu.VMEM((layers, 3, width, chan), bf16),
            pltpu.VMEM((layers, 2, 2, chan, chan), bf16),
            pltpu.VMEM((layers, width // chan, chunks, tok, chan), bf16),
            pltpu.VMEM((chunks, 2, n, WIN_C // 2, chan), bf16),
            pltpu.VMEM((chunks, 2, n, WIN_C // 2, chan), bf16),
            pltpu.VMEM((tok, width), bf16),
            pltpu.VMEM((2 * chunks, half, chan), bf16),
            pltpu.VMEM((layers, 2, 2 * chunks + 2, half, chan), bf16),
            pltpu.VMEM((layers, 2, chunks, tok, chan), bf16),
            pltpu.VMEM((layers, chunks, 2, tok, chan), bf16),
            pltpu.VMEM((layers, chunks, 2, tok, chan), bf16),
            pltpu.VMEM((chunks, tok, chan), f32),
            pltpu.VMEM((layers, heads, tok, 2 * tok), f32),
            pltpu.VMEM((layers * heads * WIN_R, LANES), f32),
            dma((layers, 3)),
            dma((layers, 2)),
            dma((layers, 2)),
            dma((layers, 2)),
            dma((chunks,)),
            dma((chunks,)),
            dma((layers, chunks, 3)),
            dma((layers, chunks, 3)),
            dma((layers, 2)),
            dma((layers, 2)),
            dma((layers, chunks)),
            dma((layers, chunks)),
            dma((layers, chunks, 2)),
            dma((layers, chunks, 2)),
            dma((chunks,)),
            dma((chunks,)),
        ],
        compiler_params=pltpu.CompilerParams(
            collective_id=0, has_side_effects=True, vmem_limit_bytes=60 * 1024 * 1024
        ),
        name="grid_attention",
    )(turned, norm_gain.astype(f32).reshape(layers, 1, width), rel_bias.reshape(-1, WIN_C), w_query, w_key, w_value, w_out)
    return jnp.transpose(out.reshape(rows_dev, columns, chan), (0, 2, 1))


def solution(mesh):
    in_specs = (
        P("sp", "tp", None),
        P(),
        P(None, None, "tp"),
        P(None, None, "tp"),
        P(None, None, "tp"),
        P(None, "tp", None),
        P(None, "tp", None, None),
    )
    out_specs = P("sp", "tp", None)
    sharded = functools.partial(jax.shard_map, mesh=mesh, in_specs=in_specs, out_specs=out_specs, check_vma=False)

    def run(token_grid, *rest):
        rows, _, columns = token_grid.shape
        n = mesh.shape["sp"]
        whole = rows == n == WIN_R and columns == 4 * WIN_C * n and mesh.shape["tp"] == 4
        return sharded(fused_body if whole else body)(token_grid, *rest)

    return run
```

```python
import functools

import jax
import jax.numpy as jnp
from jax import lax
from jax.experimental import pallas as pl
from jax.experimental.pallas import tpu as pltpu
from jax.sharding import PartitionSpec as P

HEAD_DIM = 64
WIN_R = 8
WIN_C = 16
EPS = 1e-06
LANES = 128
NEG = -1e30
MESH = pl.DeviceIdType.MESH
ORDERS = ((0, 1, 3, 2), (0, 2, 3, 1), (0, 3, 1, 2), (0, 3, 1, 2))


def attention_kernel(rows, cols, q_ref, k_ref, v_ref, kh_ref, vh_ref, base_ref, o_ref, tile_ref):
    pack = LANES // cols
    n_slots = min(rows, pack + WIN_R - 1)
    half_r = WIN_R // 2
    span = cols + WIN_C
    lane = lax.broadcasted_iota(jnp.int32, (8, LANES), 1)
    lane_q = lax.broadcasted_iota(jnp.int32, (LANES, LANES), 1)
    v_main = v_ref[...].T
    v_halo = vh_ref[...].T
    neg = jnp.full((8, LANES), NEG, jnp.float32)
    outs = [[] for _ in range(rows * cols // LANES)]
    for head in range(LANES // HEAD_DIM):
        for p in range(pack):
            own = (lane >= p * cols) & (lane < (p + 1) * cols)
            for slot in range(WIN_R):
                e = (slot + p) % rows
                start = jnp.broadcast_to(base_ref[head, slot : slot + 1, :], (8, LANES))
                start = pltpu.roll(start, 0, 1, stride=1, stride_axis=0)
                for blk in range(span // 8):
                    shift = (p * cols + 8 * blk) % LANES
                    moved = pltpu.roll(start, shift, 1) if shift else start
                    at = blk - 1 if 1 <= blk <= cols // 8 else (cols // 8 if blk == 0 else blk)
                    where = pl.ds(e * span + 8 * at, 8)
                    rest = neg if p == 0 and rows == WIN_R else tile_ref[where, :]
                    tile_ref[where, :] = jnp.where(own, moved, rest)
        for group in range(rows * cols // LANES):
            key_rows = [r for r in range(rows) if (r - group * pack + half_r) % rows < n_slots]
            q = q_ref[group * LANES : (group + 1) * LANES, :]
            mine = (lane_q >= head * HEAD_DIM) & (lane_q < (head + 1) * HEAD_DIM)
            q = jnp.where(mine, q, jnp.zeros_like(q))
            s_list = []
            contract = (((1,), (1,)), ((), ()))
            if len(key_rows) == rows:
                s_main = lax.dot_general(k_ref[...], q, contract, preferred_element_type=jnp.float32)
                s_halo = lax.dot_general(kh_ref[...], q, contract, preferred_element_type=jnp.float32)
            main_list = []
            halo_list = []
            for r in key_rows:
                e = (r - group * pack + half_r) % rows
                if len(key_rows) == rows:
                    main = s_main[r * cols : (r + 1) * cols]
                    halo = s_halo[r * WIN_C : (r + 1) * WIN_C]
                else:
                    main = lax.dot_general(
                        k_ref[r * cols : (r + 1) * cols, :], q, contract, preferred_element_type=jnp.float32
                    )
                    halo = lax.dot_general(
                        kh_ref[r * WIN_C : (r + 1) * WIN_C, :], q, contract, preferred_element_type=jnp.float32
                    )
                main_list.append(main + tile_ref[e * span : e * span + cols, :])
                halo_list.append(halo + tile_ref[e * span + cols : (e + 1) * span, :])
            main = jnp.concatenate(main_list, axis=0)
            halo = jnp.concatenate(halo_list, axis=0)
            top = jnp.maximum(jnp.max(main, axis=0, keepdims=True), jnp.max(halo, axis=0, keepdims=True))
            main = jnp.exp(main - top)
            halo = jnp.exp(halo - top)
            total = jnp.sum(main, axis=0, keepdims=True) + jnp.sum(halo, axis=0, keepdims=True)
            main = main.astype(jnp.bfloat16)
            halo = halo.astype(jnp.bfloat16)
            lo = head * HEAD_DIM
            if len(key_rows) == rows:
                vm = v_main[lo : lo + HEAD_DIM]
                vh = v_halo[lo : lo + HEAD_DIM]
            else:
                vm = jnp.concatenate([v_main[lo : lo + HEAD_DIM, r * cols : (r + 1) * cols] for r in key_rows], axis=1)
                vh = jnp.concatenate(
                    [v_halo[lo : lo + HEAD_DIM, r * WIN_C : (r + 1) * WIN_C] for r in key_rows], axis=1
                )
            mixed = jnp.dot(vm, main, preferred_element_type=jnp.float32)
            mixed = mixed + jnp.dot(vh, halo, preferred_element_type=jnp.float32)
            outs[group].append(mixed / total)
    for group in range(rows * cols // LANES):
        both = jnp.concatenate(outs[group], axis=0)
        o_ref[group * LANES : (group + 1) * LANES, :] = both.T.astype(o_ref.dtype)


def attention_kernel_init(rows, cols, *refs):
    tile_ref = refs[-1]
    tile_ref[...] = jnp.full(tile_ref.shape, NEG, jnp.float32)
    attention_kernel(rows, cols, *refs)


def attention(queries, keys, values, halo, base, rows, cols):
    tokens, channels = queries.shape
    n_slots = min(rows, LANES // cols + WIN_R - 1)
    pairs = channels // LANES
    per = LANES // HEAD_DIM
    side = halo.shape[0]
    kernel = attention_kernel if rows == WIN_R else attention_kernel_init
    return pl.pallas_call(
        functools.partial(kernel, rows, cols),
        grid=(pairs,),
        out_shape=jax.ShapeDtypeStruct((tokens, channels), jnp.bfloat16),
        in_specs=[
            pl.BlockSpec((tokens, LANES), lambda i: (0, i)),
            pl.BlockSpec((tokens, LANES), lambda i: (0, i)),
            pl.BlockSpec((tokens, LANES), lambda i: (0, i)),
            pl.BlockSpec((side, LANES), lambda i: (0, i)),
            pl.BlockSpec((side, LANES), lambda i: (0, i + pairs)),
            pl.BlockSpec((per, WIN_R, LANES), lambda i: (i, 0, 0)),
        ],
        out_specs=pl.BlockSpec((tokens, LANES), lambda i: (0, i)),
        scratch_shapes=[pltpu.VMEM((n_slots * (cols + WIN_C), LANES), jnp.float32)],
        compiler_params=pltpu.CompilerParams(vmem_limit_bytes=48 * 1024 * 1024),
        name="window_attention",
    )(queries, keys, values, halo, halo, base)


def body(token_grid, norm_gain, w_query, w_key, w_value, w_out, rel_bias):
    n = lax.axis_size("sp")
    rows_dev, channels, columns = token_grid.shape
    rows = rows_dev * n
    cols = columns // n
    tokens = rows * cols
    width = norm_gain.shape[1]
    factor = HEAD_DIM ** (-0.5)
    half_c = WIN_C // 2
    base = jnp.concatenate(
        [
            rel_bias[..., :1],
            jnp.full(rel_bias.shape[:-1] + (LANES - WIN_C,), NEG, jnp.float32),
            jnp.flip(rel_bias[..., 1:], axis=-1),
        ],
        axis=-1,
    )
    turned = jnp.transpose(token_grid, (2, 0, 1)).reshape(columns, rows_dev * channels)
    current = lax.all_to_all(turned, "sp", split_axis=0, concat_axis=0, tiled=True)
    to_right = [(i, (i + 1) % n) for i in range(n)]
    to_left = [(i, (i - 1) % n) for i in range(n)]
    for layer in range(norm_gain.shape[0]):
        gain = norm_gain[layer].astype(jnp.float32)
        raw = lax.all_gather(current, "tp", axis=1, tiled=True).astype(jnp.float32)
        scaled = (raw * gain[None, :]).astype(jnp.bfloat16)
        inverse = lax.rsqrt(jnp.sum(raw * raw, axis=1, keepdims=True) / width + EPS)

        def project(weight, scale=1.0):
            product = jnp.dot(scaled, weight[layer], preferred_element_type=jnp.float32)
            return (product * inverse).astype(jnp.bfloat16) * jnp.bfloat16(scale)

        keys = project(w_key)
        values = project(w_value)
        keyval = jnp.concatenate([keys, values], axis=1).reshape(rows, cols, 2 * channels)
        left = lax.ppermute(keyval[:, cols - half_c :], "sp", to_right)
        right = lax.ppermute(keyval[:, :half_c], "sp", to_left)
        queries = project(w_query, factor)
        halo = jnp.concatenate([left, right], axis=1).reshape(rows * WIN_C, 2 * channels)
        mixed = attention(queries, keys, values, halo, base[layer], rows, cols)
        partial = jnp.dot(mixed, w_out[layer], preferred_element_type=jnp.float32).astype(jnp.bfloat16)
        update = lax.psum_scatter(partial, "tp", scatter_dimension=1, tiled=True)
        current = (current.astype(jnp.float32) + update.astype(jnp.float32)).astype(jnp.bfloat16)
    back = lax.all_to_all(current, "sp", split_axis=0, concat_axis=0, tiled=True)
    return jnp.transpose(back.reshape(columns, rows_dev, channels), (1, 2, 0))

def unit_pairs(blocks):
    odd = [(b, (b + 1) % blocks) for b in range(1, blocks, 2)]
    even = [((b + 1) % blocks, (b + 2) % blocks) for b in range(1, blocks, 2)]
    return odd, even


def plan(layers, blocks, starts, orders):
    link, hop, near, mixed, halo_link, halo_hop = 2.82, 1.8, 2.0, 1.6, 2.8, 3.0
    odd, even = unit_pairs(blocks)
    units = [odd if l % 2 == 0 else even for l in range(layers + 1)]
    count = len(odd)
    gathered = [starts] + list(orders)

    def needs(l, i):
        wanted, sides = set(), []
        for b in units[l + 1][i]:
            for near_b in (b - 1, b, b + 1):
                if 0 <= near_b < blocks:
                    wanted.update(u for u, pair in enumerate(units[l]) if near_b in pair)
                else:
                    sides.append(near_b < 0)
        return wanted, sides

    now, wire = 0.0, 0.0
    side_wire = {True: 0.0, False: 0.0}
    own, across, relayed, done, halo, mx, sums = {}, {}, {}, set(), {}, {}, {}
    at = {kind: [0] * layers for kind in ("qkv", "attend", "project", "finish", "relay")}
    first, steps = 0, []

    def send(t, loads=1):
        nonlocal wire
        wire = max(t, wire) + loads * link
        return wire + hop

    while True:
        ready = []
        if first < count:
            ready.append((4.5 + 2.7 * first, 0, "init", 0, starts[first]))
        for l in range(layers):
            def step(kind, order):
                return order[at[kind][l]] if at[kind][l] < count else None

            i = step("finish", orders[l])
            if (l, i) in sums:
                ready.append((sums[l, i], 1, "finish", l, i))
            i = step("relay", gathered[l])
            if l == 0 and (l, i) in across:
                ready.append((across[l, i], 2, "relay", l, i))
            i = step("project", orders[l])
            if (l, i) in mx:
                ready.append((mx[l, i], 3, "project", l, i))
            i = step("attend", orders[l])
            if i is not None:
                wanted, sides = needs(l, i)
                if all((l, u) in done for u in wanted) and all((l, side) in halo for side in sides):
                    ready.append((max([0.0] + [halo[l, side] for side in sides]), 4, "attend", l, i))
            i = step("qkv", gathered[l])
            if (l, i) in relayed:
                ready.append((max(relayed[l, i], own[l, i]), 5, "qkv", l, i))
        if not ready:
            return steps
        can = [r for r in ready if r[0] <= now]
        when, _, kind, l, i = min(can, key=lambda r: r[1:]) if can else min(ready)
        now = max(now, when)
        steps.append((kind, l, i))
        if kind == "init":
            first += 1
            now += 0.18
            across[0, i], own[0, i] = send(now), now + near
            continue
        at[kind][l] += 1
        if kind == "relay":
            relayed[l, i] = now + near
        elif kind == "qkv":
            done.add((l, i))
            for side, edge in ((True, blocks - 1), (False, 0)):
                if edge in units[l][i]:
                    side_wire[side] = max(now + 0.75, side_wire[side]) + halo_link
                    halo[l, side] = side_wire[side] + halo_hop
            now += 1.02
        elif kind == "attend":
            pair = units[l + 1][i]
            now += 0.64 if pair[0] < pair[1] else 1.0
            mx[l, i] = now + mixed
        elif kind == "project":
            sums[l, i] = send(now + 0.35, 1 if l == layers - 1 else 2)
            now += 0.65
        else:
            now += 0.15
            if l < layers - 1:
                relayed[l + 1, i] = own[l + 1, i] = now + near


def mega_kernel(cfg, *refs):
    layers, n, chunks, ccols, chan, heads, width, steps = cfg
    (xt, gain, bias, wq, wk, wv, wo, out,
     w_v, wo_v, xg, xin, xo, sc, q_s, kv, mx, rs_s, rs_r, pre, tile, wide,
     w_sem, wol_sem, wor_sem, in_s, in_r, far_r, near_r, hr, mr, rsr, sent, out_r) = refs
    f32, bf16 = jnp.float32, jnp.bfloat16
    tok = ccols * WIN_R
    half = tok // 2
    sp, tp = lax.axis_index("sp"), lax.axis_index("tp")
    core, yy = lax.rem(tp, 2), lax.div(tp, 2)
    partner = yy * 2 + 1 - core
    ypeer = (1 - yy) * 2 + core
    diag = (1 - yy) * 2 + 1 - core
    deep = n // 2

    def place(dev):
        z, x = lax.div(dev, 2), lax.rem(dev, 2)
        return z + x * (n - 1 - 2 * z)

    def holder(at):
        back = lax.div(at, deep)
        return 2 * (at + back * (n - 1 - 2 * at)) + back

    mine_at = place(sp)
    right, left = holder(lax.rem(mine_at + 1, n)), holder(lax.rem(mine_at + n - 1, n))

    wo_sent, ag_sent, pair_sent, halo_sent, mx_sent, sum_sent, last_sent, out_sent = (sent.at[k] for k in range(8))

    def wait_for(some, sem):
        pltpu.make_async_copy(some, some, sem).wait()

    def remote(src, dst, ssem, rsem, dev):
        return pltpu.make_async_remote_copy(
            src_ref=src, dst_ref=dst, send_sem=ssem, recv_sem=rsem, device_id=dev, device_id_type=MESH
        )

    far_first = sorted(range(1, n), key=lambda k: -min(k, n - k))

    bar = pltpu.get_barrier_semaphore()
    for k in range(1, n):
        pl.semaphore_signal(bar, inc=1, device_id=(lax.rem(sp + k, n), tp), device_id_type=MESH)
    pl.semaphore_signal(bar, inc=1, device_id=(sp, partner), device_id_type=MESH)
    pl.semaphore_signal(bar, inc=1, device_id=(sp, ypeer), device_id_type=MESH)
    pl.semaphore_wait(bar, n + 1)

    blocks = 2 * chunks
    odd, even = unit_pairs(blocks)
    units = [odd if l % 2 == 0 else even for l in range(layers + 1)]

    def sends_in(i):
        (b0, b1), out = odd[i], []
        for k in far_first:
            to = lax.rem(sp + k, n)
            if b1 == b0 + 1:
                out.append(remote(xt.at[place(to), b0 : b0 + 2], xin.at[i, :, sp], in_s.at[i], in_r.at[i], (to, tp)))
            else:
                for j, blk in enumerate((b0, b1)):
                    out.append(remote(xt.at[place(to), blk], xin.at[i, j, sp], in_s.at[i], in_r.at[i], (to, tp)))
        return out

    def own_inputs(i):
        return [pltpu.make_async_copy(xt.at[mine_at, blk], xin.at[i, j, sp], in_r.at[i]) for j, blk in enumerate(odd[i])]

    def sent_in(i):
        wait_for(xin.at[i, :, pl.ds(0, n - 1)], in_s.at[i])

    starts = [i for kind, _, i in steps if kind == "init"]
    for i in starts[:2]:
        for c in own_inputs(i) + sends_in(i):
            c.start()

    def weight_copies(l):
        return [pltpu.make_async_copy(w.at[l], w_v.at[l, m], w_sem.at[l]) for m, w in enumerate((wk, wv, wq))]

    def cols_of(c, o):
        return pl.ds(pl.multiple_of((o * 2 + c) * chan, 128), chan)

    def own_out(l):
        return [pltpu.make_async_copy(wo.at[l, :, cols_of(core, o)], wo_v.at[l, core, o], wol_sem.at[l]) for o in range(2)]

    def partner_out(l):
        return [
            remote(wo.at[l, :, cols_of(1 - core, o)], wo_v.at[l, core, o], wo_sent, wor_sem.at[l], (sp, partner))
            for o in range(2)
        ]

    for c in weight_copies(0) + own_out(0) + partner_out(0):
        c.start()

    spread_at = lax.broadcasted_iota(jnp.int32, (ccols, LANES), 0)
    spread_to = lax.broadcasted_iota(jnp.int32, (ccols, LANES), 1)
    spread = jnp.where(lax.div(spread_to, WIN_R) == spread_at, 1.0, 0.0)
    wide[...] = jnp.dot(bias[...], spread, preferred_element_type=f32, precision=lax.Precision.HIGHEST)
    query_row = lax.broadcasted_iota(jnp.int32, (WIN_R, LANES), 0)
    key_row = lax.rem(lax.broadcasted_iota(jnp.int32, (WIN_R, LANES), 1), WIN_R)
    slot_row = lax.rem(key_row - query_row + WIN_R + WIN_R // 2, WIN_R)
    outside = jnp.full((WIN_R, LANES), NEG, f32)

    def build(at, carry):
        l, h = lax.div(at, heads), lax.rem(at, heads)
        slots = wide[pl.ds(pl.multiple_of(at * WIN_R, WIN_R), WIN_R), :]
        b = jnp.zeros((WIN_R, LANES), f32)
        for i in range(WIN_R):
            b = jnp.where(slot_row == i, slots[i : i + 1, :], b)
        b = jnp.concatenate([b, outside], axis=1)
        for qc in range(ccols):
            tile[l, h, qc * WIN_R : (qc + 1) * WIN_R, :] = pltpu.roll(b, WIN_R * qc, 1) if qc else b
        return carry

    lax.fori_loop(0, layers * heads, build, 0)

    for was, i in zip(starts, starts[2:]):
        sent_in(was)
        for c in own_inputs(i) + sends_in(i):
            c.start()

    a = lax.broadcasted_iota(jnp.int32, (tok, tok), 0)
    b = lax.broadcasted_iota(jnp.int32, (tok, tok), 1)
    same = lax.div(a, half) == lax.div(b, half)
    ra, rb = lax.rem(a, half), lax.rem(b, half)
    swap = same & (lax.div(ra, WIN_R) == lax.rem(rb, WIN_R)) & (lax.rem(ra, WIN_R) == lax.div(rb, WIN_R))
    swap = jnp.where(swap, 1.0, 0.0).astype(bf16)

    def ag_copies(l, i):
        own = xg.at[l, tp, i]
        return [
            remote(own, own, ag_sent, far_r.at[i], (sp, ypeer)),
            remote(own, own, ag_sent, near_r.at[l, i], (sp, partner)),
        ]

    def relay_copy(l, i):
        slot = xg.at[l, ypeer, i]
        return remote(slot, slot, ag_sent, near_r.at[l, i], (sp, partner))

    def ag_send(l, i):
        for c in ag_copies(l, i):
            c.start()

    def relay(l, i):
        ag_copies(l, i)[0].wait_recv()
        relay_copy(l, i).start()

    def partner_copies(l, i):
        slots = [xg.at[l, 2 * o + core, i] for o in range(2)]
        return [remote(slots[o], slots[o], pair_sent, near_r.at[l, i], (sp, partner)) for o in range(2)]

    def ag_recv(l, i):
        wait_for(xg.at[l, pl.ds(0, 2), i], near_r.at[l, i])

    def init(i):
        wait_for(xin.at[i], in_r.at[i])
        raw = xin[i].astype(f32).reshape(tok, chan).astype(bf16)
        xg[0, tp, i] = jnp.dot(swap, raw, preferred_element_type=f32).astype(bf16)
        ag_send(0, i)

    def halo_copies(l):
        return [
            remote(kv.at[l, :, 2 * chunks], kv.at[l, :, 0], halo_sent, hr.at[l, 0], (right, tp)),
            remote(kv.at[l, :, 1], kv.at[l, :, 2 * chunks + 1], halo_sent, hr.at[l, 1], (left, tp)),
        ]

    def qkv(l, i):
        ag_recv(l, i)
        total = jnp.zeros((tok, 1), f32)
        for s in range(width // chan):
            raw = xg[l, s, i].astype(f32)
            total = total + jnp.sum(raw * raw, axis=1, keepdims=True)
            sc[:, s * chan : (s + 1) * chan] = (raw * gain[l : l + 1, s * chan : (s + 1) * chan].astype(f32)).astype(bf16)
        inverse = lax.rsqrt(total / width + EPS)
        x = sc[...]
        for m in range(2):
            prod = jnp.dot(x, w_v[l, m], preferred_element_type=f32) * inverse
            prod = prod.astype(bf16)
            for j, blk in enumerate(units[l][i]):
                kv[l, m, 1 + blk] = prod[j * half : (j + 1) * half]
        if 0 in units[l][i]:
            halo_copies(l)[1].start()
        if blocks - 1 in units[l][i]:
            halo_copies(l)[0].start()
        prod = jnp.dot(x, w_v[l, 2], preferred_element_type=f32) * inverse
        prod = prod.astype(bf16) * bf16(HEAD_DIM ** (-0.5))
        for j, blk in enumerate(units[l][i]):
            q_s[blk] = prod[j * half : (j + 1) * half]

    def mx_copy(l, i):
        slot = mx.at[l, core, i]
        return remote(slot, slot, mx_sent, mr.at[l, i], (sp, partner))

    def window(l, q0, qn, k0, t0, out_at):
        rows = qn * half
        lane = lax.broadcasted_iota(jnp.int32, (rows, LANES), 1)
        ones = jnp.ones((2 * tok, LANES), bf16)
        for p in range(chan // LANES):
            at = slice(p * LANES, (p + 1) * LANES)
            q = q_s[q0 : q0 + qn, :, at].reshape(rows, LANES)
            key = kv[l, 0, k0 : k0 + 4, :, at].reshape(2 * tok, LANES)
            val = kv[l, 1, k0 : k0 + 4, :, at].reshape(2 * tok, LANES)
            val = jnp.concatenate([val, ones], axis=1)
            res = []
            for hh in range(2):
                mine = (lane >= hh * HEAD_DIM) & (lane < (hh + 1) * HEAD_DIM)
                qm = jnp.where(mine, q, jnp.zeros_like(q))
                s = lax.dot_general(qm, key, (((1,), (1,)), ((), ())), preferred_element_type=f32)
                s = s + tile[l, 2 * p + hh, t0 : t0 + rows]
                e = jnp.exp(s - jnp.max(s, axis=1, keepdims=True)).astype(bf16)
                o = jnp.dot(e, val, preferred_element_type=f32)
                res.append(o[:, :LANES] / o[:, LANES:])
            out_at[:, at] = jnp.where(lane < HEAD_DIM, res[0], res[1]).astype(bf16)

    def attend(l, i):
        b0, b1 = units[l + 1][i]
        if b1 == b0 + 1:
            window(l, b0, 2, b0, 0, mx.at[l, core, i])
        else:
            window(l, b0, 1, b0 - 1, half, mx.at[l, core, i, :half])
            window(l, b1, 1, b1, 0, mx.at[l, core, i, half:])
        mx_copy(l, i).start()

    def rs_copy(l, i, o):
        done = last_sent if l == layers - 1 else sum_sent
        return remote(rs_s.at[l, i, o], rs_r.at[l, i, o], done, rsr.at[l, i, o], (sp, ypeer))

    def old(l, i, slot):
        parts = []
        for blk in units[l + 1][i]:
            u = [blk in pair for pair in units[l]].index(True)
            k = units[l][u].index(blk)
            parts.append(xg[l, slot, u, k * half : (k + 1) * half])
        return jnp.concatenate(parts, axis=0).astype(f32)

    def project(l, i):
        mx_copy(l, i).wait_recv()
        a0, a1 = mx[l, 0, i], mx[l, 1, i]

        def part(o):
            return jnp.dot(a0, wo_v[l, 0, o], preferred_element_type=f32) + jnp.dot(
                a1, wo_v[l, 1, o], preferred_element_type=f32
            )

        if l == layers - 1:
            rs_s[l, i, 0] = part(1 - yy).astype(bf16)
            rs_copy(l, i, 0).start()
            pre[i] = old(l, i, tp) + part(yy)
        else:
            for o in range(2):
                rs_s[l, i, o] = part(o).astype(bf16)
                rs_copy(l, i, o).start()

    def updated(i):
        rs_copy(layers - 1, i, 0).wait_recv()
        return (pre[i] + rs_r[layers - 1, i, 0].astype(f32)).astype(bf16)

    def finish(l, i):
        for o in range(2):
            rs_copy(l, i, o).wait_recv()
            slot = 2 * o + core
            both = rs_s[l, i, o].astype(f32) + rs_r[l, i, o].astype(f32)
            xg[l + 1, slot, i] = (old(l, i, slot) + both).astype(bf16)
            partner_copies(l + 1, i)[o].start()

    def out_copies(i):
        (b0, b1), out_list = units[layers][i], []
        for k in far_first:
            to = lax.rem(sp + k, n)
            if b1 == b0 + 1:
                out_list.append(remote(xo.at[i, :, to], out.at[mine_at, b0 : b0 + 2], out_sent, out_r.at[0], (to, tp)))
            else:
                for j, blk in enumerate((b0, b1)):
                    out_list.append(remote(xo.at[i, j, to], out.at[mine_at, blk], out_sent, out_r.at[0], (to, tp)))
        return out_list

    def own_results(i):
        return [
            pltpu.make_async_copy(xo.at[i, j, sp], out.at[mine_at, blk], out_r.at[0])
            for j, blk in enumerate(units[layers][i])
        ]

    def finish_last(i):
        rows = jnp.dot(swap, updated(i), preferred_element_type=f32)
        xo[i] = rows.reshape(2, n, half // n, chan).astype(bf16)
        for c in out_copies(i):
            c.start()
        for c in own_results(i):
            c.start()

    def leave(l, i):
        if l == layers - 1:
            finish_last(i)
        else:
            finish(l, i)

    def load(l, what):
        for c in what(l):
            c.start()

    seen = set()

    def once(*key):
        fresh = key not in seen
        seen.add(key)
        return fresh

    for kind, l, i in steps:
        if kind == "init":
            init(i)
            if l + 1 < layers and once("load", l + 1):
                load(l + 1, weight_copies)
                load(l + 1, own_out)
        elif kind == "relay":
            relay(l, i)
        elif kind == "qkv":
            if once("weights", l):
                wait_for(w_v.at[l], w_sem.at[l])
            qkv(l, i)
        elif kind == "attend":
            for blk in units[l + 1][i]:
                if blk in (0, blocks - 1) and once("halo", l, blk):
                    halo_copies(l)[0 if blk == 0 else 1].wait_recv()
            attend(l, i)
        elif kind == "project":
            if once("out", l):
                wait_for(wo_v.at[l, core], wol_sem.at[l])
                wait_for(wo_v.at[l, 1 - core], wor_sem.at[l])
            project(l, i)
            if l + 1 < layers and once("load out", l + 1):
                load(l + 1, partner_out)
            if l + 2 < layers and once("load", l + 2):
                load(l + 2, weight_copies)
                load(l + 2, own_out)
        else:
            leave(l, i)

    wait_for(xo, out_r.at[0])
    wait_for(xo.at[:, :, pl.ds(0, n - 1)], out_sent)
    for i in starts[2:]:
        sent_in(i)
    wait_for(wo_v.at[:, 0], wo_sent)
    wait_for(xg.at[0, pl.ds(0, 3)], ag_sent)
    wait_for(xg.at[pl.ds(1, layers - 1), pl.ds(0, 2)], pair_sent)
    wait_for(kv.at[:, :, pl.ds(0, 2)], halo_sent)
    wait_for(mx.at[:, 0], mx_sent)
    wait_for(rs_s.at[pl.ds(0, layers - 1)], sum_sent)
    wait_for(rs_s.at[layers - 1, :, 0], last_sent)


def fused_body(token_grid, norm_gain, w_query, w_key, w_value, w_out, rel_bias):
    n = lax.axis_size("sp")
    rows_dev, chan, columns = token_grid.shape
    layers, width = norm_gain.shape
    heads = rel_bias.shape[1]
    chunks = columns // n // WIN_C
    bf16, f32 = jnp.bfloat16, jnp.float32
    turned = jnp.transpose(token_grid, (0, 2, 1)).reshape(n, 2 * chunks, WIN_C // 2, chan)
    tok = WIN_C * WIN_R
    half = tok // 2
    cfg = (layers, n, chunks, WIN_C, chan, heads, width, plan(layers, 2 * chunks, ORDERS[0], ORDERS[1:]))
    hbm, vmem = pl.BlockSpec(memory_space=pl.ANY), pl.BlockSpec(memory_space=pltpu.VMEM)
    dma = pltpu.SemaphoreType.DMA
    out = pl.pallas_call(
        functools.partial(mega_kernel, cfg),
        out_shape=jax.ShapeDtypeStruct((n, 2 * chunks, WIN_C // 2, chan), bf16),
        in_specs=[hbm, vmem, vmem] + [hbm] * 4,
        out_specs=hbm,
        scratch_shapes=[
            pltpu.VMEM((layers, 3, width, chan), bf16),
            pltpu.VMEM((layers, 2, 2, chan, chan), bf16),
            pltpu.VMEM((layers, width // chan, chunks, tok, chan), bf16),
            pltpu.VMEM((chunks, 2, n, WIN_C // 2, chan), bf16),
            pltpu.VMEM((chunks, 2, n, WIN_C // 2, chan), bf16),
            pltpu.VMEM((tok, width), bf16),
            pltpu.VMEM((2 * chunks, half, chan), bf16),
            pltpu.VMEM((layers, 2, 2 * chunks + 2, half, chan), bf16),
            pltpu.VMEM((layers, 2, chunks, tok, chan), bf16),
            pltpu.VMEM((layers, chunks, 2, tok, chan), bf16),
            pltpu.VMEM((layers, chunks, 2, tok, chan), bf16),
            pltpu.VMEM((chunks, tok, chan), f32),
            pltpu.VMEM((layers, heads, tok, 2 * tok), f32),
            pltpu.VMEM((layers * heads * WIN_R, LANES), f32),
            dma((layers,)),
            dma((layers,)),
            dma((layers,)),
            dma((chunks,)),
            dma((chunks,)),
            dma((chunks,)),
            dma((layers, chunks)),
            dma((layers, 2)),
            dma((layers, chunks)),
            dma((layers, chunks, 2)),
            dma((8,)),
            dma((1,)),
        ],
        compiler_params=pltpu.CompilerParams(
            collective_id=0, has_side_effects=True, vmem_limit_bytes=52 * 1024 * 1024
        ),
        name="grid_attention",
    )(turned, norm_gain, rel_bias.reshape(-1, WIN_C), w_query, w_key, w_value, w_out)
    return jnp.transpose(out.reshape(rows_dev, columns, chan), (0, 2, 1))


def solution(mesh):
    in_specs = (
        P("sp", "tp", None),
        P(),
        P(None, None, "tp"),
        P(None, None, "tp"),
        P(None, None, "tp"),
        P(None, "tp", None),
        P(None, "tp", None, None),
    )
    out_specs = P("sp", "tp", None)
    sharded = functools.partial(jax.shard_map, mesh=mesh, in_specs=in_specs, out_specs=out_specs, check_vma=False)

    def run(token_grid, *rest):
        rows, _, columns = token_grid.shape
        n = mesh.shape["sp"]
        whole = rows == n == WIN_R and columns == len(ORDERS[0]) * WIN_C * n and mesh.shape["tp"] == 4
        whole = whole and rest[0].shape[0] == len(ORDERS) - 1
        return sharded(fused_body if whole else body)(token_grid, *rest)

    return run
```

```python
import functools

import jax
import jax.numpy as jnp
from jax import lax
from jax.experimental import pallas as pl
from jax.experimental.pallas import tpu as pltpu
from jax.sharding import PartitionSpec as P

HEAD_DIM = 64
WIN_R = 8
WIN_C = 16
EPS = 1e-06
LANES = 128
NEG = -1e30
MESH = pl.DeviceIdType.MESH
ORDERS = ((3, 0, 1, 2), (3, 2, 0, 1), (0, 3, 2, 1), (2, 3, 0, 1))


def attention_kernel(rows, cols, q_ref, k_ref, v_ref, kh_ref, vh_ref, base_ref, o_ref, tile_ref):
    pack = LANES // cols
    n_slots = min(rows, pack + WIN_R - 1)
    half_r = WIN_R // 2
    span = cols + WIN_C
    lane = lax.broadcasted_iota(jnp.int32, (8, LANES), 1)
    lane_q = lax.broadcasted_iota(jnp.int32, (LANES, LANES), 1)
    v_main = v_ref[...].T
    v_halo = vh_ref[...].T
    neg = jnp.full((8, LANES), NEG, jnp.float32)
    outs = [[] for _ in range(rows * cols // LANES)]
    for head in range(LANES // HEAD_DIM):
        for p in range(pack):
            own = (lane >= p * cols) & (lane < (p + 1) * cols)
            for slot in range(WIN_R):
                e = (slot + p) % rows
                start = jnp.broadcast_to(base_ref[head, slot : slot + 1, :], (8, LANES))
                start = pltpu.roll(start, 0, 1, stride=1, stride_axis=0)
                for blk in range(span // 8):
                    shift = (p * cols + 8 * blk) % LANES
                    moved = pltpu.roll(start, shift, 1) if shift else start
                    at = blk - 1 if 1 <= blk <= cols // 8 else (cols // 8 if blk == 0 else blk)
                    where = pl.ds(e * span + 8 * at, 8)
                    rest = neg if p == 0 and rows == WIN_R else tile_ref[where, :]
                    tile_ref[where, :] = jnp.where(own, moved, rest)
        for group in range(rows * cols // LANES):
            key_rows = [r for r in range(rows) if (r - group * pack + half_r) % rows < n_slots]
            q = q_ref[group * LANES : (group + 1) * LANES, :]
            mine = (lane_q >= head * HEAD_DIM) & (lane_q < (head + 1) * HEAD_DIM)
            q = jnp.where(mine, q, jnp.zeros_like(q))
            s_list = []
            contract = (((1,), (1,)), ((), ()))
            if len(key_rows) == rows:
                s_main = lax.dot_general(k_ref[...], q, contract, preferred_element_type=jnp.float32)
                s_halo = lax.dot_general(kh_ref[...], q, contract, preferred_element_type=jnp.float32)
            main_list = []
            halo_list = []
            for r in key_rows:
                e = (r - group * pack + half_r) % rows
                if len(key_rows) == rows:
                    main = s_main[r * cols : (r + 1) * cols]
                    halo = s_halo[r * WIN_C : (r + 1) * WIN_C]
                else:
                    main = lax.dot_general(
                        k_ref[r * cols : (r + 1) * cols, :], q, contract, preferred_element_type=jnp.float32
                    )
                    halo = lax.dot_general(
                        kh_ref[r * WIN_C : (r + 1) * WIN_C, :], q, contract, preferred_element_type=jnp.float32
                    )
                main_list.append(main + tile_ref[e * span : e * span + cols, :])
                halo_list.append(halo + tile_ref[e * span + cols : (e + 1) * span, :])
            main = jnp.concatenate(main_list, axis=0)
            halo = jnp.concatenate(halo_list, axis=0)
            top = jnp.maximum(jnp.max(main, axis=0, keepdims=True), jnp.max(halo, axis=0, keepdims=True))
            main = jnp.exp(main - top)
            halo = jnp.exp(halo - top)
            total = jnp.sum(main, axis=0, keepdims=True) + jnp.sum(halo, axis=0, keepdims=True)
            main = main.astype(jnp.bfloat16)
            halo = halo.astype(jnp.bfloat16)
            lo = head * HEAD_DIM
            if len(key_rows) == rows:
                vm = v_main[lo : lo + HEAD_DIM]
                vh = v_halo[lo : lo + HEAD_DIM]
            else:
                vm = jnp.concatenate([v_main[lo : lo + HEAD_DIM, r * cols : (r + 1) * cols] for r in key_rows], axis=1)
                vh = jnp.concatenate(
                    [v_halo[lo : lo + HEAD_DIM, r * WIN_C : (r + 1) * WIN_C] for r in key_rows], axis=1
                )
            mixed = jnp.dot(vm, main, preferred_element_type=jnp.float32)
            mixed = mixed + jnp.dot(vh, halo, preferred_element_type=jnp.float32)
            outs[group].append(mixed / total)
    for group in range(rows * cols // LANES):
        both = jnp.concatenate(outs[group], axis=0)
        o_ref[group * LANES : (group + 1) * LANES, :] = both.T.astype(o_ref.dtype)


def attention_kernel_init(rows, cols, *refs):
    tile_ref = refs[-1]
    tile_ref[...] = jnp.full(tile_ref.shape, NEG, jnp.float32)
    attention_kernel(rows, cols, *refs)


def attention(queries, keys, values, halo, base, rows, cols):
    tokens, channels = queries.shape
    n_slots = min(rows, LANES // cols + WIN_R - 1)
    pairs = channels // LANES
    per = LANES // HEAD_DIM
    side = halo.shape[0]
    kernel = attention_kernel if rows == WIN_R else attention_kernel_init
    return pl.pallas_call(
        functools.partial(kernel, rows, cols),
        grid=(pairs,),
        out_shape=jax.ShapeDtypeStruct((tokens, channels), jnp.bfloat16),
        in_specs=[
            pl.BlockSpec((tokens, LANES), lambda i: (0, i)),
            pl.BlockSpec((tokens, LANES), lambda i: (0, i)),
            pl.BlockSpec((tokens, LANES), lambda i: (0, i)),
            pl.BlockSpec((side, LANES), lambda i: (0, i)),
            pl.BlockSpec((side, LANES), lambda i: (0, i + pairs)),
            pl.BlockSpec((per, WIN_R, LANES), lambda i: (i, 0, 0)),
        ],
        out_specs=pl.BlockSpec((tokens, LANES), lambda i: (0, i)),
        scratch_shapes=[pltpu.VMEM((n_slots * (cols + WIN_C), LANES), jnp.float32)],
        compiler_params=pltpu.CompilerParams(vmem_limit_bytes=48 * 1024 * 1024),
        name="window_attention",
    )(queries, keys, values, halo, halo, base)


def body(token_grid, norm_gain, w_query, w_key, w_value, w_out, rel_bias):
    n = lax.axis_size("sp")
    rows_dev, channels, columns = token_grid.shape
    rows = rows_dev * n
    cols = columns // n
    tokens = rows * cols
    width = norm_gain.shape[1]
    factor = HEAD_DIM ** (-0.5)
    half_c = WIN_C // 2
    base = jnp.concatenate(
        [
            rel_bias[..., :1],
            jnp.full(rel_bias.shape[:-1] + (LANES - WIN_C,), NEG, jnp.float32),
            jnp.flip(rel_bias[..., 1:], axis=-1),
        ],
        axis=-1,
    )
    turned = jnp.transpose(token_grid, (2, 0, 1)).reshape(columns, rows_dev * channels)
    current = lax.all_to_all(turned, "sp", split_axis=0, concat_axis=0, tiled=True)
    to_right = [(i, (i + 1) % n) for i in range(n)]
    to_left = [(i, (i - 1) % n) for i in range(n)]
    for layer in range(norm_gain.shape[0]):
        gain = norm_gain[layer].astype(jnp.float32)
        raw = lax.all_gather(current, "tp", axis=1, tiled=True).astype(jnp.float32)
        scaled = (raw * gain[None, :]).astype(jnp.bfloat16)
        inverse = lax.rsqrt(jnp.sum(raw * raw, axis=1, keepdims=True) / width + EPS)

        def project(weight, scale=1.0):
            product = jnp.dot(scaled, weight[layer], preferred_element_type=jnp.float32)
            return (product * inverse).astype(jnp.bfloat16) * jnp.bfloat16(scale)

        keys = project(w_key)
        values = project(w_value)
        keyval = jnp.concatenate([keys, values], axis=1).reshape(rows, cols, 2 * channels)
        left = lax.ppermute(keyval[:, cols - half_c :], "sp", to_right)
        right = lax.ppermute(keyval[:, :half_c], "sp", to_left)
        queries = project(w_query, factor)
        halo = jnp.concatenate([left, right], axis=1).reshape(rows * WIN_C, 2 * channels)
        mixed = attention(queries, keys, values, halo, base[layer], rows, cols)
        partial = jnp.dot(mixed, w_out[layer], preferred_element_type=jnp.float32).astype(jnp.bfloat16)
        update = lax.psum_scatter(partial, "tp", scatter_dimension=1, tiled=True)
        current = (current.astype(jnp.float32) + update.astype(jnp.float32)).astype(jnp.bfloat16)
    back = lax.all_to_all(current, "sp", split_axis=0, concat_axis=0, tiled=True)
    return jnp.transpose(back.reshape(columns, rows_dev, channels), (1, 2, 0))

def unit_pairs(blocks):
    odd = [(b, (b + 1) % blocks) for b in range(1, blocks, 2)]
    even = [((b + 1) % blocks, (b + 2) % blocks) for b in range(1, blocks, 2)]
    return odd, even


def plan(layers, blocks, starts, orders):
    link, hop, near, mixed, halo_link, halo_hop = 2.82, 2.0, 2.6, 1.5, 2.8, 2.8
    arrival = (4.6, 8.6, 11.0, 13.5)
    odd, even = unit_pairs(blocks)
    units = [odd if l % 2 == 0 else even for l in range(layers + 1)]
    count = len(odd)
    gathered = [starts] + list(orders)

    def needs(l, i):
        wanted, sides = set(), []
        for b in units[l + 1][i]:
            for near_b in (b - 1, b, b + 1):
                if 0 <= near_b < blocks:
                    wanted.update(u for u, pair in enumerate(units[l]) if near_b in pair)
                else:
                    sides.append(near_b < 0)
        return wanted, sides

    now, wire = 0.0, 0.0
    side_wire = {True: 0.0, False: 0.0}
    own, across, relayed, done, halo, mx, sums = {}, {}, {}, set(), {}, {}, {}
    at = {kind: [0] * layers for kind in ("qkv", "attend", "project", "finish", "relay")}
    first, steps = 0, []

    def send(t, loads=1):
        nonlocal wire
        wire = max(t, wire) + loads * link
        return wire + hop

    while True:
        ready = []
        if first < count:
            ready.append((arrival[first], 0, "init", 0, starts[first]))
        for l in range(layers):
            def step(kind, order):
                return order[at[kind][l]] if at[kind][l] < count else None

            i = step("finish", orders[l])
            if (l, i) in sums:
                ready.append((sums[l, i], 1, "finish", l, i))
            i = step("relay", gathered[l])
            if l == 0 and (l, i) in across:
                ready.append((across[l, i], 2, "relay", l, i))
            i = step("project", orders[l])
            if (l, i) in mx:
                ready.append((mx[l, i], 3, "project", l, i))
            i = step("attend", orders[l])
            if i is not None:
                wanted, sides = needs(l, i)
                if all((l, u) in done for u in wanted) and all((l, side) in halo for side in sides):
                    ready.append((max([0.0] + [halo[l, side] for side in sides]), 4, "attend", l, i))
            i = step("qkv", gathered[l])
            if (l, i) in relayed:
                ready.append((max(relayed[l, i], own[l, i]), 5, "qkv", l, i))
        if not ready:
            return steps
        can = [r for r in ready if r[0] <= now]
        idle = [r for r in ready if r[2] == "project" and wire <= max(now, r[0]) and r[0] <= now + mixed]
        when, _, kind, l, i = min(idle) if idle else min(can, key=lambda r: r[1:]) if can else min(ready)
        now = max(now, when)
        steps.append((kind, l, i))
        if kind == "init":
            first += 1
            now += 0.18
            across[0, i], own[0, i] = send(now), now + near
            continue
        at[kind][l] += 1
        if kind == "relay":
            relayed[l, i] = now + near
        elif kind == "qkv":
            done.add((l, i))
            for side, edge in ((True, blocks - 1), (False, 0)):
                if edge in units[l][i]:
                    side_wire[side] = max(now + 0.75, side_wire[side]) + halo_link
                    halo[l, side] = side_wire[side] + halo_hop
            now += 1.02
        elif kind == "attend":
            pair = units[l + 1][i]
            now += 0.64 if pair[0] < pair[1] else 1.0
            mx[l, i] = now + mixed
        elif kind == "project":
            sums[l, i] = send(now + 0.35, 1 if l == layers - 1 else 2)
            now += 0.65
        else:
            now += 0.15
            if l < layers - 1:
                relayed[l + 1, i] = own[l + 1, i] = now + near


def mega_kernel(cfg, *refs):
    layers, n, chunks, ccols, chan, heads, width, steps = cfg
    (xt, gain, bias, wq, wk, wv, wo, out,
     w_v, wo_v, xg, xin, xo, sc, q_s, kv, mx, rs_s, rs_r, pre, tile, wide,
     w_sem, wol_sem, wor_sem, in_s, in_r, far_r, near_r, hr, mr, rsr, sent, out_r) = refs
    f32, bf16 = jnp.float32, jnp.bfloat16
    tok = ccols * WIN_R
    half = tok // 2
    sp, tp = lax.axis_index("sp"), lax.axis_index("tp")
    core, yy = lax.rem(tp, 2), lax.div(tp, 2)
    partner = yy * 2 + 1 - core
    ypeer = (1 - yy) * 2 + core
    diag = (1 - yy) * 2 + 1 - core
    deep = n // 2

    def place(dev):
        z, x = lax.div(dev, 2), lax.rem(dev, 2)
        return z + x * (n - 1 - 2 * z)

    def holder(at):
        back = lax.div(at, deep)
        return 2 * (at + back * (n - 1 - 2 * at)) + back

    mine_at = place(sp)
    right, left = holder(lax.rem(mine_at + 1, n)), holder(lax.rem(mine_at + n - 1, n))

    wo_sent, ag_sent, pair_sent, halo_sent, mx_sent, sum_sent, last_sent, out_sent = (sent.at[k] for k in range(8))

    def wait_for(some, sem):
        pltpu.make_async_copy(some, some, sem).wait()

    def remote(src, dst, ssem, rsem, dev):
        return pltpu.make_async_remote_copy(
            src_ref=src, dst_ref=dst, send_sem=ssem, recv_sem=rsem, device_id=dev, device_id_type=MESH
        )

    far_first = sorted(range(1, n), key=lambda k: -min(k, n - k))

    bar = pltpu.get_barrier_semaphore()
    for k in range(1, n):
        pl.semaphore_signal(bar, inc=1, device_id=(lax.rem(sp + k, n), tp), device_id_type=MESH)
    pl.semaphore_signal(bar, inc=1, device_id=(sp, partner), device_id_type=MESH)
    pl.semaphore_signal(bar, inc=1, device_id=(sp, ypeer), device_id_type=MESH)
    pl.semaphore_wait(bar, n + 1)

    blocks = 2 * chunks
    odd, even = unit_pairs(blocks)
    units = [odd if l % 2 == 0 else even for l in range(layers + 1)]

    def sends_in(i):
        (b0, b1), out = odd[i], []
        for k in far_first:
            to = lax.rem(sp + k, n)
            if b1 == b0 + 1:
                out.append(remote(xt.at[place(to), b0 : b0 + 2], xin.at[i, :, sp], in_s.at[i], in_r.at[i], (to, tp)))
            else:
                for j, blk in enumerate((b0, b1)):
                    out.append(remote(xt.at[place(to), blk], xin.at[i, j, sp], in_s.at[i], in_r.at[i], (to, tp)))
        return out

    def own_inputs(i):
        return [pltpu.make_async_copy(xt.at[mine_at, blk], xin.at[i, j, sp], in_r.at[i]) for j, blk in enumerate(odd[i])]

    def sent_in(i):
        wait_for(xin.at[i, :, pl.ds(0, n - 1)], in_s.at[i])

    starts = [i for kind, _, i in steps if kind == "init"]
    for i in starts[:2]:
        for c in own_inputs(i) + sends_in(i):
            c.start()

    def weight_copies(l):
        return [pltpu.make_async_copy(w.at[l], w_v.at[l, m], w_sem.at[l]) for m, w in enumerate((wk, wv, wq))]

    def cols_of(c, o):
        return pl.ds(pl.multiple_of((o * 2 + c) * chan, 128), chan)

    def own_out(l):
        return [pltpu.make_async_copy(wo.at[l, :, cols_of(core, o)], wo_v.at[l, core, o], wol_sem.at[l]) for o in range(2)]

    def partner_out(l):
        return [
            remote(wo.at[l, :, cols_of(1 - core, o)], wo_v.at[l, core, o], wo_sent, wor_sem.at[l], (sp, partner))
            for o in range(2)
        ]

    for c in weight_copies(0) + own_out(0) + partner_out(0):
        c.start()

    spread_at = lax.broadcasted_iota(jnp.int32, (ccols, LANES), 0)
    spread_to = lax.broadcasted_iota(jnp.int32, (ccols, LANES), 1)
    spread = jnp.where(lax.div(spread_to, WIN_R) == spread_at, 1.0, 0.0)
    wide[...] = jnp.dot(bias[...], spread, preferred_element_type=f32, precision=lax.Precision.HIGHEST)
    query_row = lax.broadcasted_iota(jnp.int32, (WIN_R, LANES), 0)
    key_row = lax.rem(lax.broadcasted_iota(jnp.int32, (WIN_R, LANES), 1), WIN_R)
    slot_row = lax.rem(key_row - query_row + WIN_R + WIN_R // 2, WIN_R)
    outside = jnp.full((WIN_R, LANES), NEG, f32)

    def build(at, carry):
        l, h = lax.div(at, heads), lax.rem(at, heads)
        slots = wide[pl.ds(pl.multiple_of(at * WIN_R, WIN_R), WIN_R), :]
        b = jnp.zeros((WIN_R, LANES), f32)
        for i in range(WIN_R):
            b = jnp.where(slot_row == i, slots[i : i + 1, :], b)
        b = jnp.concatenate([b, outside], axis=1)
        for qc in range(ccols):
            tile[l, h, qc * WIN_R : (qc + 1) * WIN_R, :] = pltpu.roll(b, WIN_R * qc, 1) if qc else b
        return carry

    lax.fori_loop(0, layers * heads, build, 0)

    for was, i in zip(starts, starts[2:]):
        sent_in(was)
        for c in own_inputs(i) + sends_in(i):
            c.start()

    a = lax.broadcasted_iota(jnp.int32, (tok, tok), 0)
    b = lax.broadcasted_iota(jnp.int32, (tok, tok), 1)
    same = lax.div(a, half) == lax.div(b, half)
    ra, rb = lax.rem(a, half), lax.rem(b, half)
    swap = same & (lax.div(ra, WIN_R) == lax.rem(rb, WIN_R)) & (lax.rem(ra, WIN_R) == lax.div(rb, WIN_R))
    swap = jnp.where(swap, 1.0, 0.0).astype(bf16)

    def ag_copies(l, i):
        own = xg.at[l, tp, i]
        return [
            remote(own, own, ag_sent, far_r.at[i], (sp, ypeer)),
            remote(own, own, ag_sent, near_r.at[l, i], (sp, partner)),
        ]

    def relay_copy(l, i):
        slot = xg.at[l, ypeer, i]
        return remote(slot, slot, ag_sent, near_r.at[l, i], (sp, partner))

    def ag_send(l, i):
        for c in ag_copies(l, i):
            c.start()

    def relay(l, i):
        ag_copies(l, i)[0].wait_recv()
        relay_copy(l, i).start()

    def partner_copies(l, i):
        slots = [xg.at[l, 2 * o + core, i] for o in range(2)]
        return [remote(slots[o], slots[o], pair_sent, near_r.at[l, i], (sp, partner)) for o in range(2)]

    def ag_recv(l, i):
        wait_for(xg.at[l, pl.ds(0, 2), i], near_r.at[l, i])

    def init(i):
        wait_for(xin.at[i], in_r.at[i])
        raw = xin[i].astype(f32).reshape(tok, chan).astype(bf16)
        xg[0, tp, i] = jnp.dot(swap, raw, preferred_element_type=f32).astype(bf16)
        ag_send(0, i)

    def halo_copies(l):
        return [
            remote(kv.at[l, :, 2 * chunks], kv.at[l, :, 0], halo_sent, hr.at[l, 0], (right, tp)),
            remote(kv.at[l, :, 1], kv.at[l, :, 2 * chunks + 1], halo_sent, hr.at[l, 1], (left, tp)),
        ]

    def qkv(l, i):
        ag_recv(l, i)
        total = jnp.zeros((tok, 1), f32)
        for s in range(width // chan):
            raw = xg[l, s, i].astype(f32)
            total = total + jnp.sum(raw * raw, axis=1, keepdims=True)
            sc[:, s * chan : (s + 1) * chan] = (raw * gain[l : l + 1, s * chan : (s + 1) * chan].astype(f32)).astype(bf16)
        inverse = lax.rsqrt(total / width + EPS)
        x = sc[...]
        for m in range(2):
            prod = jnp.dot(x, w_v[l, m], preferred_element_type=f32) * inverse
            prod = prod.astype(bf16)
            for j, blk in enumerate(units[l][i]):
                kv[l, m, 1 + blk] = prod[j * half : (j + 1) * half]
        if 0 in units[l][i]:
            halo_copies(l)[1].start()
        if blocks - 1 in units[l][i]:
            halo_copies(l)[0].start()
        prod = jnp.dot(x, w_v[l, 2], preferred_element_type=f32) * inverse
        prod = prod.astype(bf16) * bf16(HEAD_DIM ** (-0.5))
        for j, blk in enumerate(units[l][i]):
            q_s[blk] = prod[j * half : (j + 1) * half]

    def mx_copy(l, i):
        slot = mx.at[l, core, i]
        return remote(slot, slot, mx_sent, mr.at[l, i], (sp, partner))

    def window(l, q0, qn, k0, t0, out_at):
        rows = qn * half
        lane = lax.broadcasted_iota(jnp.int32, (rows, LANES), 1)
        ones = jnp.ones((2 * tok, LANES), bf16)
        for p in range(chan // LANES):
            at = slice(p * LANES, (p + 1) * LANES)
            q = q_s[q0 : q0 + qn, :, at].reshape(rows, LANES)
            key = kv[l, 0, k0 : k0 + 4, :, at].reshape(2 * tok, LANES)
            val = kv[l, 1, k0 : k0 + 4, :, at].reshape(2 * tok, LANES)
            val = jnp.concatenate([val, ones], axis=1)
            res = []
            for hh in range(2):
                mine = (lane >= hh * HEAD_DIM) & (lane < (hh + 1) * HEAD_DIM)
                qm = jnp.where(mine, q, jnp.zeros_like(q))
                s = lax.dot_general(qm, key, (((1,), (1,)), ((), ())), preferred_element_type=f32)
                s = s + tile[l, 2 * p + hh, t0 : t0 + rows]
                e = jnp.exp(s - jnp.max(s, axis=1, keepdims=True)).astype(bf16)
                o = jnp.dot(e, val, preferred_element_type=f32)
                res.append(o[:, :LANES] / o[:, LANES:])
            out_at[:, at] = jnp.where(lane < HEAD_DIM, res[0], res[1]).astype(bf16)

    def attend(l, i):
        b0, b1 = units[l + 1][i]
        if b1 == b0 + 1:
            window(l, b0, 2, b0, 0, mx.at[l, core, i])
        else:
            window(l, b0, 1, b0 - 1, half, mx.at[l, core, i, :half])
            window(l, b1, 1, b1, 0, mx.at[l, core, i, half:])
        mx_copy(l, i).start()

    def rs_copy(l, i, o):
        done = last_sent if l == layers - 1 else sum_sent
        return remote(rs_s.at[l, i, o], rs_r.at[l, i, o], done, rsr.at[l, i, o], (sp, ypeer))

    def old(l, i, slot):
        parts = []
        for blk in units[l + 1][i]:
            u = [blk in pair for pair in units[l]].index(True)
            k = units[l][u].index(blk)
            parts.append(xg[l, slot, u, k * half : (k + 1) * half])
        return jnp.concatenate(parts, axis=0).astype(f32)

    def project(l, i):
        mx_copy(l, i).wait_recv()
        a0, a1 = mx[l, 0, i], mx[l, 1, i]

        def part(o):
            return jnp.dot(a0, wo_v[l, 0, o], preferred_element_type=f32) + jnp.dot(
                a1, wo_v[l, 1, o], preferred_element_type=f32
            )

        if l == layers - 1:
            rs_s[l, i, 0] = part(1 - yy).astype(bf16)
            rs_copy(l, i, 0).start()
            pre[i] = old(l, i, tp) + part(yy)
        else:
            for o in range(2):
                rs_s[l, i, o] = part(o).astype(bf16)
                rs_copy(l, i, o).start()

    def updated(i):
        rs_copy(layers - 1, i, 0).wait_recv()
        return (pre[i] + rs_r[layers - 1, i, 0].astype(f32)).astype(bf16)

    def finish(l, i):
        for o in range(2):
            rs_copy(l, i, o).wait_recv()
            slot = 2 * o + core
            both = rs_s[l, i, o].astype(f32) + rs_r[l, i, o].astype(f32)
            xg[l + 1, slot, i] = (old(l, i, slot) + both).astype(bf16)
            partner_copies(l + 1, i)[o].start()

    def out_copies(i):
        (b0, b1), out_list = units[layers][i], []
        for k in far_first:
            to = lax.rem(sp + k, n)
            if b1 == b0 + 1:
                out_list.append(remote(xo.at[i, :, to], out.at[mine_at, b0 : b0 + 2], out_sent, out_r.at[0], (to, tp)))
            else:
                for j, blk in enumerate((b0, b1)):
                    out_list.append(remote(xo.at[i, j, to], out.at[mine_at, blk], out_sent, out_r.at[0], (to, tp)))
        return out_list

    def own_results(i):
        return [
            pltpu.make_async_copy(xo.at[i, j, sp], out.at[mine_at, blk], out_r.at[0])
            for j, blk in enumerate(units[layers][i])
        ]

    def finish_last(i):
        rows = jnp.dot(swap, updated(i), preferred_element_type=f32)
        xo[i] = rows.reshape(2, n, half // n, chan).astype(bf16)
        for c in out_copies(i):
            c.start()
        for c in own_results(i):
            c.start()

    def leave(l, i):
        if l == layers - 1:
            finish_last(i)
        else:
            finish(l, i)

    def load(l, what):
        for c in what(l):
            c.start()

    seen = set()

    def once(*key):
        fresh = key not in seen
        seen.add(key)
        return fresh

    for kind, l, i in steps:
        if kind == "init":
            init(i)
            if i == starts[-1] and l + 1 < layers and once("load", l + 1):
                load(l + 1, weight_copies)
                load(l + 1, own_out)
        elif kind == "relay":
            relay(l, i)
        elif kind == "qkv":
            if once("weights", l):
                wait_for(w_v.at[l], w_sem.at[l])
            qkv(l, i)
        elif kind == "attend":
            for blk in units[l + 1][i]:
                if blk in (0, blocks - 1) and once("halo", l, blk):
                    halo_copies(l)[0 if blk == 0 else 1].wait_recv()
            attend(l, i)
        elif kind == "project":
            if once("out", l):
                wait_for(wo_v.at[l, core], wol_sem.at[l])
                wait_for(wo_v.at[l, 1 - core], wor_sem.at[l])
            project(l, i)
            if l + 1 < layers and once("load out", l + 1):
                load(l + 1, partner_out)
            if l + 2 < layers and once("load", l + 2):
                load(l + 2, weight_copies)
                load(l + 2, own_out)
        else:
            leave(l, i)

    wait_for(xo, out_r.at[0])
    wait_for(xo.at[:, :, pl.ds(0, n - 1)], out_sent)
    for i in starts[2:]:
        sent_in(i)
    wait_for(wo_v.at[:, 0], wo_sent)
    wait_for(xg.at[0, pl.ds(0, 3)], ag_sent)
    wait_for(xg.at[pl.ds(1, layers - 1), pl.ds(0, 2)], pair_sent)
    wait_for(kv.at[:, :, pl.ds(0, 2)], halo_sent)
    wait_for(mx.at[:, 0], mx_sent)
    wait_for(rs_s.at[pl.ds(0, layers - 1)], sum_sent)
    wait_for(rs_s.at[layers - 1, :, 0], last_sent)


def fused_body(token_grid, norm_gain, w_query, w_key, w_value, w_out, rel_bias):
    n = lax.axis_size("sp")
    rows_dev, chan, columns = token_grid.shape
    layers, width = norm_gain.shape
    heads = rel_bias.shape[1]
    chunks = columns // n // WIN_C
    bf16, f32 = jnp.bfloat16, jnp.float32
    turned = jnp.transpose(token_grid, (0, 2, 1)).reshape(n, 2 * chunks, WIN_C // 2, chan)
    tok = WIN_C * WIN_R
    half = tok // 2
    cfg = (layers, n, chunks, WIN_C, chan, heads, width, plan(layers, 2 * chunks, ORDERS[0], ORDERS[1:]))
    hbm, vmem = pl.BlockSpec(memory_space=pl.ANY), pl.BlockSpec(memory_space=pltpu.VMEM)
    dma = pltpu.SemaphoreType.DMA
    out = pl.pallas_call(
        functools.partial(mega_kernel, cfg),
        out_shape=jax.ShapeDtypeStruct((n, 2 * chunks, WIN_C // 2, chan), bf16),
        in_specs=[hbm, vmem, vmem] + [hbm] * 4,
        out_specs=hbm,
        scratch_shapes=[
            pltpu.VMEM((layers, 3, width, chan), bf16),
            pltpu.VMEM((layers, 2, 2, chan, chan), bf16),
            pltpu.VMEM((layers, width // chan, chunks, tok, chan), bf16),
            pltpu.VMEM((chunks, 2, n, WIN_C // 2, chan), bf16),
            pltpu.VMEM((chunks, 2, n, WIN_C // 2, chan), bf16),
            pltpu.VMEM((tok, width), bf16),
            pltpu.VMEM((2 * chunks, half, chan), bf16),
            pltpu.VMEM((layers, 2, 2 * chunks + 2, half, chan), bf16),
            pltpu.VMEM((layers, 2, chunks, tok, chan), bf16),
            pltpu.VMEM((layers, chunks, 2, tok, chan), bf16),
            pltpu.VMEM((layers, chunks, 2, tok, chan), bf16),
            pltpu.VMEM((chunks, tok, chan), f32),
            pltpu.VMEM((layers, heads, tok, 2 * tok), f32),
            pltpu.VMEM((layers * heads * WIN_R, LANES), f32),
            dma((layers,)),
            dma((layers,)),
            dma((layers,)),
            dma((chunks,)),
            dma((chunks,)),
            dma((chunks,)),
            dma((layers, chunks)),
            dma((layers, 2)),
            dma((layers, chunks)),
            dma((layers, chunks, 2)),
            dma((8,)),
            dma((1,)),
        ],
        compiler_params=pltpu.CompilerParams(
            collective_id=0, has_side_effects=True, vmem_limit_bytes=52 * 1024 * 1024
        ),
        name="grid_attention",
    )(turned, norm_gain, rel_bias.reshape(-1, WIN_C), w_query, w_key, w_value, w_out)
    return jnp.transpose(out.reshape(rows_dev, columns, chan), (0, 2, 1))


def solution(mesh):
    in_specs = (
        P("sp", "tp", None),
        P(),
        P(None, None, "tp"),
        P(None, None, "tp"),
        P(None, None, "tp"),
        P(None, "tp", None),
        P(None, "tp", None, None),
    )
    out_specs = P("sp", "tp", None)
    sharded = functools.partial(jax.shard_map, mesh=mesh, in_specs=in_specs, out_specs=out_specs, check_vma=False)

    def run(token_grid, *rest):
        rows, _, columns = token_grid.shape
        n = mesh.shape["sp"]
        whole = rows == n == WIN_R and columns == len(ORDERS[0]) * WIN_C * n and mesh.shape["tp"] == 4
        whole = whole and rest[0].shape[0] == len(ORDERS) - 1
        return sharded(fused_body if whole else body)(token_grid, *rest)

    return run
```
